32 devices in a mesh: fs: 4 (over y, x), tp: 8 (over z, core).
Axes of the slice: x: 2, y: 2, z: 4, core: 2. Of those that a mesh axis runs over, the one named last changes fastest.
Arguments:
- features: bfloat16 [8192, 2048], P('fs', 'tp'), may hold values from -6 to 6
- gate_cotangent: bfloat16 [8192, 4096], P('fs', 'tp'), may hold values from -0.059814453 to 0.059814453
- gate_basis: bfloat16 [2048, 128], replicated, may hold values from -0.125 to 0.125
- gate_master: float32 [2048, 4096], P('fs', 'tp'), may hold values from -6 to 6
- gate_first: float32 [128, 4096], P('fs', 'tp'), may hold values from -144 to 144
- gate_second: float32 [128, 4096], P('fs', 'tp'), may hold values from 0.2 to 4
- input_cotangent: bfloat16 [8192, 4096], P('fs', 'tp'), may hold values from -0.059814453 to 0.059814453
- input_basis: bfloat16 [2048, 128], replicated, may hold values from -0.125 to 0.125
- input_master: float32 [2048, 4096], P('fs', 'tp'), may hold values from -6 to 6
- input_first: float32 [128, 4096], P('fs', 'tp'), may hold values from -144 to 144
- input_second: float32 [128, 4096], P('fs', 'tp'), may hold values from 0.2 to 4
- state_cotangent: bfloat16 [8192, 1024], P('fs', 'tp'), may hold values from -0.059814453 to 0.059814453
- state_basis: bfloat16 [2048, 128], replicated, may hold values from -0.125 to 0.125
- state_master: float32 [2048, 1024], P('fs', 'tp'), may hold values from -6 to 6
- state_first: float32 [128, 1024], P('fs', 'tp'), may hold values from -144 to 144
- state_second: float32 [128, 1024], P('fs', 'tp'), may hold values from 0.2 to 4
Outputs:
- gate_update: float32 [2048, 4096], P('fs', 'tp')
- gate_master_next: float32 [2048, 4096], P('fs', 'tp')
- gate_first_next: float32 [128, 4096], P('fs', 'tp')
- gate_second_next: float32 [128, 4096], P('fs', 'tp')
- gate_copy: bfloat16 [2048, 4096], P(None, 'tp')
- input_update: float32 [2048, 4096], P('fs', 'tp')
- input_master_next: float32 [2048, 4096], P('fs', 'tp')
- input_first_next: float32 [128, 4096], P('fs', 'tp')
- input_second_next: float32 [128, 4096], P('fs', 'tp')
- input_copy: bfloat16 [2048, 4096], P(None, 'tp')
- state_update: float32 [2048, 1024], P('fs', 'tp')
- state_master_next: float32 [2048, 1024], P('fs', 'tp')
- state_first_next: float32 [128, 1024], P('fs', 'tp')
- state_second_next: float32 [128, 1024], P('fs', 'tp')
- state_copy: bfloat16 [2048, 1024], P(None, 'tp')
The draws below stay inside these ranges and needn't reach their ends.
All inputs are finite; a program needn't handle non-finite values.
Results may differ from the reference program's by a relative error of at most 0.001.
Values may be sent and summed in bfloat16 or wider, within the bound.
A program may use at most 64 MiB of HBM per device.

```python
import math
import jax
import jax.numpy as jnp
from jax import lax

D = 2048
INNER = 4096
STATE_COLS = 1024
RANK = 128
TOKENS = 8192


def rising_moment(key, rows, columns):
    base = jnp.clip(jax.random.normal(key, (rows, columns), jnp.float32), -4.0, 4.0)
    row_pos = jnp.arange(rows, dtype=jnp.float32) / rows
    col_pos = jnp.arange(columns, dtype=jnp.float32) / columns
    growth = math.log(3.0)
    return base * jnp.exp(growth * (row_pos[:, None] + col_pos[None, :]))


def draw_gate_first(key, part):
    return rising_moment(jax.random.fold_in(key, 11), RANK, INNER)


def draw_input_first(key, part):
    return rising_moment(jax.random.fold_in(key, 12), RANK, INNER)


def draw_state_first(key, part):
    return rising_moment(jax.random.fold_in(key, 13), RANK, STATE_COLS)


def levels(key, dims, pieces, least, top_value):
    gain = 1.0
    for axis_at, shards_of in pieces:
        steps = jax.random.uniform(jax.random.fold_in(jax.random.fold_in(key, 6), axis_at), (shards_of,), jnp.float32, least / len(pieces), top_value / len(pieces))
        gain = gain * jnp.repeat(jnp.exp(steps), dims[axis_at] // shards_of).reshape((-1,) + (1,) * (len(dims) - 1 - axis_at))
    return gain


def gaussian(rng, extent, width, bound, cuts=(), kind=jnp.bfloat16):
    level = levels(rng, extent, cuts, -0.22, 0.18) if cuts else 1.0
    entries = jax.random.normal(rng, extent, jnp.float32) * width * level
    return jnp.minimum(jnp.maximum(entries, -bound), bound).astype(kind)


def setup_inputs(seed: int = 0) -> dict:
    key_of = jax.random.split(jax.random.key(seed), 17)
    return {
        "features": gaussian(key_of[0], (TOKENS, D), 1.0, 6.0, ((0, 4), (1, 8))),
        "gate_cotangent": gaussian(key_of[1], (TOKENS, INNER), 0.01, 0.059814453, ((0, 4), (1, 8))),
        "gate_basis": gaussian(key_of[2], (D, RANK), D ** -0.5, 0.125),
        "gate_master": gaussian(key_of[3], (D, INNER), 1.0, 6.0, ((0, 4), (1, 8)), jnp.float32),
        "gate_first": draw_gate_first(jax.random.fold_in(key_of[16], 71), 0),
        "gate_second": jnp.clip(jnp.exp(math.log(4.0) - 2.9957323 * jax.random.uniform(key_of[5], (RANK, INNER), jnp.float32) ** levels(key_of[5], (RANK, INNER), ((0, 4), (1, 8)), -0.2, 0.2)), 0.2, 4.0),
        "input_cotangent": gaussian(key_of[6], (TOKENS, INNER), 0.01, 0.059814453, ((0, 4), (1, 8))),
        "input_basis": gaussian(key_of[7], (D, RANK), D ** -0.5, 0.125),
        "input_master": gaussian(key_of[8], (D, INNER), 1.0, 6.0, ((0, 4), (1, 8)), jnp.float32),
        "input_first": draw_input_first(jax.random.fold_in(key_of[16], 71), 0),
        "input_second": jnp.clip(jnp.exp(math.log(4.0) - 2.9957323 * jax.random.uniform(key_of[10], (RANK, INNER), jnp.float32) ** levels(key_of[10], (RANK, INNER), ((0, 4), (1, 8)), -0.2, 0.2)), 0.2, 4.0),
        "state_cotangent": gaussian(key_of[11], (TOKENS, STATE_COLS), 0.01, 0.059814453, ((0, 4), (1, 8))),
        "state_basis": gaussian(key_of[12], (D, RANK), D ** -0.5, 0.125),
        "state_master": gaussian(key_of[13], (D, STATE_COLS), 1.0, 6.0, ((0, 4), (1, 8)), jnp.float32),
        "state_first": draw_state_first(jax.random.fold_in(key_of[16], 71), 0),
        "state_second": jnp.clip(jnp.exp(math.log(4.0) - 2.9957323 * jax.random.uniform(key_of[15], (RANK, STATE_COLS), jnp.float32) ** levels(key_of[15], (RANK, STATE_COLS), ((0, 4), (1, 8)), -0.2, 0.2)), 0.2, 4.0),
    }


def one_matrix(features, cotangent, basis, master, first, second):
    gradient = jnp.dot(features.T, cotangent, preferred_element_type=jnp.float32)
    basis_wide = basis.astype(jnp.float32)
    projected = jnp.dot(basis_wide.T, gradient, precision=lax.Precision.HIGHEST)
    first_next = 0.8 * first + 0.2 * projected
    second_next = 0.9 * second + 0.1 * projected * projected
    direction = first_next / jnp.sqrt(second_next)
    scale = lax.rsqrt(jnp.mean(direction * direction) + 1e-06)
    update = jnp.dot(basis_wide, direction, precision=lax.Precision.HIGHEST) * scale
    master_next = master - 0.05 * update
    return (update, master_next, first_next, second_next, master_next.astype(jnp.bfloat16))

def reference(features, gate_cotangent, gate_basis, gate_master, gate_first, gate_second, input_cotangent, input_basis, input_master, input_first, input_second, state_cotangent, state_basis, state_master, state_first, state_second):
    gate_out = one_matrix(features, gate_cotangent, gate_basis, gate_master, gate_first, gate_second)
    input_out = one_matrix(features, input_cotangent, input_basis, input_master, input_first, input_second)
    state_out = one_matrix(features, state_cotangent, state_basis, state_master, state_first, state_second)
    return (gate_out[0], gate_out[1], gate_out[2], gate_out[3], gate_out[4], input_out[0], input_out[1], input_out[2], input_out[3], input_out[4], state_out[0], state_out[1], state_out[2], state_out[3], state_out[4])
```

```python
import functools

import jax
import jax.numpy as jnp
from jax import lax
from jax.experimental import pallas as pl
from jax.experimental.pallas import tpu as pltpu
from jax.sharding import PartitionSpec as P

MESH = pl.DeviceIdType.MESH
PIECES = 4
SKEW = 2
AFTER = (0, 1, 4, 7, 9, 13)
F32, BF16 = jnp.float32, jnp.bfloat16


def kernel(n, tp, *refs):
    feat_in = refs[0]
    cot_in, basis_in, master_in, first_in, second_in = (refs[1 + i : 16 : 5] for i in range(5))
    upd, mas, fir, sec, cop = (refs[16 + i : 31 : 5] for i in range(5))
    (feat, fsib, cot, basis, master, first, second, parts, up_in, dn_in, up_snd, dn_snd,
     tot, sib, proj, rs_in, direction, sums,
     load_sem, z_send, z_recv, sib_send, sib_recv, rs_send, rs_recv,
     ag_send, ag_recv, sq_send, sq_recv, bulk_send, bulk_recv) = (
        refs[31], refs[32], refs[33:36], refs[36:39], refs[39:42], refs[42:45], refs[45:48],
        *refs[48:53], refs[53], refs[54], refs[55:58], refs[58:61], refs[61:64], refs[64],
        *refs[65:])

    f, t = lax.axis_index("fs"), lax.axis_index("tp")
    zs = tp // 2
    z, c = t // 2, lax.rem(t, 2)
    mate = 2 * z + 1 - c
    half = feat.shape[0]
    width = feat.shape[1]
    rows_dev = master[0].shape[0]
    rank = proj[0].shape[0]
    rb = rank // n
    piece = half // PIECES
    count = 3 * PIECES

    def remote(src, dst, ssem, rsem, **dev):
        return pltpu.make_async_remote_copy(
            src_ref=src, dst_ref=dst, send_sem=ssem, recv_sem=rsem, device_id=dev, device_id_type=MESH
        )

    def load(src, dst, i):
        cp = pltpu.make_async_copy(src, dst, load_sem.at[i])
        cp.start()
        return cp

    my_half = pl.multiple_of(c * half, half)
    mate_half = pl.multiple_of((1 - c) * half, half)
    loads = [load(feat_in.at[pl.ds(my_half, half)], feat, 0)]
    loads += [load(basis_in[k], basis[k], 1 + k) for k in range(3)]
    loads += [load(cot_in[k], cot[k], 4 + k) for k in range(3)]
    loads += [load(first_in[k], first[k], 7 + k) for k in range(3)]
    loads += [load(second_in[k], second[k], 10 + k) for k in range(3)]
    loads += [load(master_in[k], master[k], 13 + k) for k in range(3)]

    barrier = pltpu.get_barrier_semaphore()
    for d in range(1, n):
        pl.semaphore_signal(barrier, inc=1, device_id={"fs": lax.rem(f + d, n)}, device_id_type=MESH)
    for d in range(1, tp):
        pl.semaphore_signal(barrier, inc=1, device_id={"tp": lax.rem(t + d, tp)}, device_id_type=MESH)
    pl.semaphore_wait(barrier, n + tp - 2)

    share = remote(feat_in.at[pl.ds(mate_half, half)], fsib, sib_send.at[3], sib_recv.at[3], tp=mate)
    share.start()

    @pl.when(z == 0)
    def _():
        up_in[...] = jnp.zeros_like(up_in)

    @pl.when(z == zs - 1)
    def _():
        dn_in[...] = jnp.zeros_like(dn_in)

    for cp in loads[:4]:
        cp.wait()
    mine = pl.ds(pl.multiple_of(t * width, width), width)
    theirs = pl.ds(pl.multiple_of(mate * width, width), width)
    share.wait()
    for k in range(3):
        own = jnp.dot(feat[...], basis[k][mine, :], preferred_element_type=F32)
        own += jnp.dot(fsib[...], basis[k][theirs, :], preferred_element_type=F32)
        for j in range(PIECES):
            parts[k * PIECES + j] = own[j * piece : (j + 1) * piece]

    def hop(j, has_src, has_dst, src_in, snd, lane, to):
        @pl.when((j >= 0) & (j < count))
        def _():
            jj = jnp.clip(j, 0, count - 1)
            copy = remote(snd.at[jj], src_in.at[jj], z_send.at[lane, jj], z_recv.at[lane, jj], tp=to)

            @pl.when(has_src)
            def _():
                copy.wait_recv()

            @pl.when(has_dst)
            def _():
                snd[jj] = (parts[jj] + src_in[jj].astype(F32)).astype(BF16)
                copy.start()

    above = jnp.minimum(t + 2, tp - 2 + c)
    below = jnp.maximum(t - 2, c)

    def z_step(step):
        hop(step - SKEW * z, z > 0, z < zs - 1, up_in, up_snd, 0, above)
        hop(step - SKEW * (zs - 1 - z), z < zs - 1, z > 0, dn_in, dn_snd, 1, below)

    mate_copy = [remote(tot.at[k], sib.at[k], sib_send.at[k], sib_recv.at[k], tp=mate) for k in range(3)]

    def act_total(k):
        for j in range(PIECES):
            i = k * PIECES + j
            whole = parts[i] + up_in[i].astype(F32) + dn_in[i].astype(F32)
            tot[k, j * piece : (j + 1) * piece, :] = whole.astype(BF16)
        mate_copy[k].start()

    def contract(a, b):
        return lax.dot_general(a, b, (((0,), (0,)), ((), ())), preferred_element_type=F32)

    def rows_of(i):
        return pl.ds(pl.multiple_of(i * rb, rb), rb)

    def rs_copy(k, d):
        peer = lax.rem(f + d, n)
        return remote(proj[k].at[rows_of(peer)], rs_in[k].at[d - 1], rs_send.at[k, d - 1], rs_recv.at[k, d - 1], fs=peer)

    def ag_copy(k, d, whose):
        peer = lax.rem(f + d, n)
        r = direction[k].at[rows_of(whose)]
        return remote(r, r, ag_send.at[k, d - 1], ag_recv.at[k, d - 1], fs=peer)

    def sq_copy(k, d, whose):
        peer = lax.rem(t + d, tp)
        r = sums.at[k, whose]
        return remote(r, r, sq_send.at[k, d - 1], sq_recv.at[k, d - 1], tp=peer)

    def act_project(k):
        loads[4 + k].wait()
        acc = contract(tot[k], cot[k][pl.ds(my_half, half), :])
        mate_copy[k].wait_recv()
        proj[k][...] = acc + contract(sib[k], cot[k][pl.ds(mate_half, half), :])
        for d in range(1, n):
            rs_copy(k, d).start()

    def act_moment(k):
        loads[7 + k].wait()
        loads[10 + k].wait()
        r = proj[k][rows_of(f), :]
        for d in range(1, n):
            rs_copy(k, d).wait_recv()
            r = r + rs_in[k][d - 1]
        a = 0.8 * first[k][...] + 0.2 * r
        b = 0.9 * second[k][...] + 0.1 * r * r
        fir[k][...] = a
        sec[k][...] = b
        direction[k][rows_of(f), :] = a / jnp.sqrt(b)
        for d in range(1, n):
            ag_copy(k, d, f).start()

    rows = pl.ds(pl.multiple_of(f * rows_dev, rows_dev), rows_dev)

    def act_direction(k):
        for d in range(1, n):
            ag_copy(k, d, lax.rem(f - d + n, n)).wait_recv()
        whole = direction[k][...]
        sums[k, t] = jnp.full((8, 128), jnp.sum(whole * whole), F32)
        for d in range(1, tp):
            sq_copy(k, d, t).start()
        high = whole.astype(BF16)
        low = (whole - high.astype(F32)).astype(BF16)
        base = basis[k][rows, :]
        upd[k][...] = jnp.dot(
            jnp.concatenate([base, base], axis=1),
            jnp.concatenate([high, low], axis=0),
            preferred_element_type=F32,
        )

    hrow = rows_dev // 2

    def block(k, owner, h):
        return cop[k].at[pl.ds(pl.multiple_of(owner * rows_dev + h * hrow, hrow), hrow)]

    x_peer = f + 1 - 2 * lax.rem(f, 2)
    y_peer = lax.rem(f + 2, 4)
    diag = lax.rem(x_peer + 2, 4)

    def bulk(k, lane, owner, h, to):
        b = block(k, owner, h)
        return remote(b, b, bulk_send.at[k, lane], bulk_recv.at[k, lane], fs=to)

    def act_finish(k):
        loads[13 + k].wait()
        for d in range(1, tp):
            sq_copy(k, d, lax.rem(t - d + tp, tp)).wait_recv()
        total = jnp.sum(sums[k], axis=0)[0:1, 0:1]
        entries = rank * upd[k].shape[1] * tp
        scale = lax.rsqrt(total / entries + 1e-06)
        update = upd[k][...] * scale
        upd[k][...] = update
        new = master[k][...] - 0.05 * update
        mas[k][...] = new
        cop[k][rows, :] = new.astype(BF16)
        if n == 4:
            for h in range(2):
                bulk(k, h, f, h, x_peer).start()
                bulk(k, 3 - h, f, 1 - h, y_peer).start()
        else:
            for d in range(1, n):
                for h in range(2):
                    bulk(k, 2 * (d - 1) + h, f, h, lax.rem(f + d, n)).start()

    def act_forward(k):
        if n == 4:
            bulk(k, 0, x_peer, 0, x_peer).wait_recv()
            bulk(k, 4, x_peer, 0, y_peer).start()
            bulk(k, 3, y_peer, 1, y_peer).wait_recv()
            bulk(k, 5, y_peer, 1, x_peer).start()

    def act_arrive(k):
        if n == 4:
            for i, (lane, owner, h) in enumerate(((1, x_peer, 1), (2, y_peer, 0), (4, diag, 0), (5, diag, 1))):
                bulk(k, lane, owner, h, x_peer).wait_recv()
        else:
            for d in range(1, n):
                for h in range(2):
                    owner = lax.rem(f - d + n, n)
                    lane = 2 * (d - 1) + h
                    bulk(k, lane, owner, h, owner).wait_recv()

    todo = {}
    for k in range(3):
        base = (k + 1) * PIECES - 1 + SKEW * (zs - 1)
        for after, act in zip(AFTER, (act_total, act_project, act_moment, act_direction, act_finish, act_forward)):
            todo.setdefault(base + after, []).append((act, k))
    steps = count + SKEW * (zs - 1)
    for step in range(max(max(todo) + 1, steps)):
        if step < steps:
            z_step(step)
        for act, k in sorted(todo.get(step, ()), key=lambda item: -item[1]):
            act(k)
    for k in range(3):
        act_arrive(k)

    for k in range(3):
        mate_copy[k].wait_send()
        for d in range(1, n):
            rs_copy(k, d).wait_send()
            ag_copy(k, d, f).wait_send()
        for d in range(1, tp):
            sq_copy(k, d, t).wait_send()
        if n == 4:
            for h in range(2):
                bulk(k, h, f, h, x_peer).wait_send()
                bulk(k, 3 - h, f, 1 - h, y_peer).wait_send()
            bulk(k, 4, x_peer, 0, y_peer).wait_send()
            bulk(k, 5, y_peer, 1, x_peer).wait_send()
        else:
            for d in range(1, n):
                for h in range(2):
                    bulk(k, 2 * (d - 1) + h, f, h, lax.rem(f + d, n)).wait_send()
    for j in range(count):
        @pl.when(z < zs - 1)
        def _():
            remote(up_snd.at[j], up_in.at[j], z_send.at[0, j], z_recv.at[0, j], tp=above).wait_send()

        @pl.when(z > 0)
        def _():
            remote(dn_snd.at[j], dn_in.at[j], z_send.at[1, j], z_recv.at[1, j], tp=below).wait_send()


def emit(*refs):
    copies = [pltpu.make_async_copy(refs[i], refs[15 + i], refs[30].at[i]) for i in range(15)]
    for cp in copies:
        cp.start()
    for cp in copies:
        cp.wait()


def shards(n, tp, *args):
    features = args[0]
    cots, bases, masters, firsts, seconds = (args[1 + i : 16 : 5] for i in range(5))
    tokens, width = features.shape
    rank = bases[0].shape[1]
    rows_dev = masters[0].shape[0]
    whole_rows = rows_dev * n
    half = tokens // 2
    count = 3 * PIECES
    piece = half // PIECES
    cols = [a.shape[1] for a in cots]

    outs = []
    for k in range(3):
        outs += [
            pltpu.VMEM(masters[k].shape, F32),
            pltpu.VMEM(masters[k].shape, F32),
            pltpu.VMEM(firsts[k].shape, F32),
            pltpu.VMEM(firsts[k].shape, F32),
            pltpu.VMEM((whole_rows, cols[k]), BF16),
        ]
    like = lambda arrays: [pltpu.VMEM(a.shape, a.dtype) for a in arrays]
    lanes = 6 if n == 4 else 2 * (n - 1)
    dma = lambda *shape: pltpu.SemaphoreType.DMA(shape)
    scratch = (
        [pltpu.VMEM((half, width), BF16)] * 2
        + like(cots)
        + like(bases)
        + like(masters)
        + like(firsts)
        + like(seconds)
        + [pltpu.VMEM((count, piece, rank), F32)]
        + [pltpu.VMEM((count, piece, rank), BF16)] * 4
        + [pltpu.VMEM((3, half, rank), BF16)] * 2
        + [pltpu.VMEM((rank, w), F32) for w in cols]
        + [pltpu.VMEM((n - 1, rank // n, w), F32) for w in cols]
        + [pltpu.VMEM((rank, w), F32) for w in cols]
        + [pltpu.VMEM((3, tp, 8, 128), F32)]
        + [dma(16), dma(2, count), dma(2, count), dma(4), dma(4)]
        + [dma(3, n - 1)] * 4
        + [dma(3, tp - 1)] * 2
        + [dma(3, lanes)] * 2
    )
    held = pl.pallas_call(
        functools.partial(kernel, n, tp),
        out_shape=outs,
        in_specs=[pl.BlockSpec(memory_space=pltpu.HBM)] * 16,
        out_specs=[pl.BlockSpec(memory_space=pltpu.VMEM)] * 15,
        scratch_shapes=scratch,
        compiler_params=pltpu.CompilerParams(
            collective_id=0, has_side_effects=True, vmem_limit_bytes=54 * 1024 * 1024
        ),
    )(*args)
    return pl.pallas_call(
        emit,
        out_shape=[jax.ShapeDtypeStruct(a.shape, a.dtype) for a in held],
        in_specs=[pl.BlockSpec(memory_space=pltpu.VMEM)] * 15,
        out_specs=[pl.BlockSpec(memory_space=pltpu.HBM)] * 15,
        scratch_shapes=[pltpu.SemaphoreType.DMA((15,))],
        compiler_params=pltpu.CompilerParams(vmem_limit_bytes=16 * 1024 * 1024),
    )(*held)


def solution(mesh):
    split = P("fs", "tp")
    return jax.shard_map(
        functools.partial(shards, mesh.shape["fs"], mesh.shape["tp"]),
        mesh=mesh,
        in_specs=(split,) + (split, P(), split, split, split) * 3,
        out_specs=(split, split, split, split, P(None, "tp")) * 3,
        check_vma=False,
    )
```

```python
import functools

import jax
import jax.numpy as jnp
from jax import lax
from jax.experimental import pallas as pl
from jax.experimental.pallas import tpu as pltpu
from jax.sharding import PartitionSpec as P

MESH = pl.DeviceIdType.MESH
PIECES = 8
SKEW = 4
EARLY = (0, 192, 512)
EARLY_ROWS = (32, 32, 128)
LATE_PAIRS = (2, 1, 1)
START_PAIRS = 4
TAIL = (
    (-4, "relay", 0),
    (-2, "relay", 1),
    (0, "relay", 2),
    (1, "own", 4),
    (7, "total", 0),
    (8, "project", 0),
    (8.5, "relay", 3),
    (13, "moment", 0),
    (15, "total", 1),
    (16, "project", 1),
    (16.5, "relay", 4),
    (17, "tally", 0),
    (20, "direction", 0),
    (22, "moment", 1),
    (22.1, "finish", 0),
    (22.2, "send", 0, 0),
    (23, "total", 2),
    (23.2, "project", 2),
    (23.4, "send", 0, 1),
    (23.5, "tally", 1),
    (24, "direction", 1),
    (26, "finish", 1),
    (27, "forward", 0, 0),
    (27.5, "moment", 2),
    (28.1, "send", 1, 0),
    (29, "forward", 0, 1),
    (29.5, "tally", 2),
    (29.6, "direction", 2),
    (29.7, "forward", 1, 0),
    (30, "finish", 2),
    (30.1, "local", 2),
    (32, "local", 1),
    (33, "arrive", 0),
    (33, "arrive", 1),
)
PLAIN = (
    (7, "total"),
    (8, "project"),
    (13, "moment"),
    (17, "tally"),
    (21, "direction"),
    (23, "finish"),
    (23.1, "send"),
    (60, "arrive"),
)
F32, BF16 = jnp.float32, jnp.bfloat16


def plan(n, rows_dev):
    early = [min(e, rows_dev) if n == 4 else 0 for e in EARLY]
    pairs = []
    for k in (2, 1, 0):
        for at in range(0, early[k], 2 * EARLY_ROWS[k]):
            pairs.append((k, at, EARLY_ROWS[k]))
    return early, pairs


def kernel(n, tp, *refs):
    feat_in = refs[0]
    cot_in, basis_in, master_in, first_in, second_in = (refs[1 + i : 16 : 5] for i in range(5))
    upd, mas, fir, sec, cop = (refs[16 + i : 31 : 5] for i in range(5))
    (feats, fsib, cot, basis, master, first, second, parts, up_in, dn_in, up_snd, dn_snd,
     tot, sib, proj, rs_out, rs_in, direction, wide, shares, sums,
     load_sem, z_send, z_recv, sib_send, sib_recv, rs_send, rs_recv,
     ag_send, ag_recv, part_send, part_recv, sq_send, sq_recv, bulk_send, bulk_recv, early_send, early_recv) = (
        refs[31], refs[32], refs[33:36], refs[36:39], refs[39:42], refs[42:45], refs[45:48],
        *refs[48:53], refs[53], refs[54], refs[55:58], refs[58:61], refs[61:64], refs[64:67],
        refs[67:70], refs[70], refs[71], *refs[72:])

    f, t = lax.axis_index("fs"), lax.axis_index("tp")
    zs = tp // 2
    z, c = t // 2, lax.rem(t, 2)
    mate = 2 * z + 1 - c
    half = feats.shape[0] // 2
    width = feats.shape[1]
    rows_dev = master[0].shape[0]
    rank = proj[0].shape[0]
    rb = rank // n
    piece = half // PIECES
    count = 3 * PIECES
    early, pairs = plan(n, rows_dev)

    def remote(src, dst, ssem, rsem, **dev):
        return pltpu.make_async_remote_copy(
            src_ref=src, dst_ref=dst, send_sem=ssem, recv_sem=rsem, device_id=dev, device_id_type=MESH
        )

    def load(src, dst, i):
        cp = pltpu.make_async_copy(src, dst, load_sem.at[i])
        cp.start()
        return cp

    my_half = pl.multiple_of(c * half, half)
    mate_half = pl.multiple_of((1 - c) * half, half)
    loads = [load(feat_in, feats, 0)]
    loads += [load(basis_in[k], basis[k], 1 + k) for k in range(3)]
    heads = [k for k in (2, 1, 0) if early[k]]
    order = heads + [k for k in range(3) if k not in heads]
    grown = {k: load(master_in[k], master[k], 13 + k) for k in heads}
    loads += [load(cot_in[k], cot[k], 4 + k) for k in range(3)]
    loads += [load(first_in[k], first[k], 7 + k) for k in range(3)]
    loads += [load(second_in[k], second[k], 10 + k) for k in range(3)]
    grown.update({k: load(master_in[k], master[k], 13 + k) for k in order if k not in heads})
    loads += [grown[k] for k in range(3)]

    barrier = pltpu.get_barrier_semaphore()
    for d in range(1, n):
        pl.semaphore_signal(barrier, inc=1, device_id={"fs": lax.rem(f + d, n)}, device_id_type=MESH)
    for d in range(1, tp):
        pl.semaphore_signal(barrier, inc=1, device_id={"tp": lax.rem(t + d, tp)}, device_id_type=MESH)

    @pl.when(z == 0)
    def _():
        up_in[...] = jnp.zeros_like(up_in)

    @pl.when(z == zs - 1)
    def _():
        dn_in[...] = jnp.zeros_like(dn_in)

    for cp in loads[:4]:
        cp.wait()
    mine = pl.ds(pl.multiple_of(t * width, width), width)
    theirs = pl.ds(pl.multiple_of(mate * width, width), width)

    def pieces_of(k):
        return pl.ds(k * PIECES, PIECES)

    for k in range(3):
        own = jnp.dot(feats[pl.ds(my_half, half), :], basis[k][mine, :], preferred_element_type=F32)
        parts[pieces_of(k)] = own.reshape(PIECES, piece, rank)
    pl.semaphore_wait(barrier, n + tp - 2)

    share = remote(feats.at[pl.ds(mate_half, half)], fsib, sib_send.at[3], sib_recv.at[3], tp=mate)
    share.start()

    x_peer = f + 1 - 2 * lax.rem(f, 2)
    y_peer = lax.rem(f + 2, 4)
    diag = lax.rem(x_peer + 2, 4)

    def early_copy(p, lane, owner, to):
        k, at, size = pairs[p]
        r = pl.ds(at + size * (lane in (1, 3, 5)), size)
        src = master[k].at[r] if lane < 4 else wide[k].at[owner, r]
        return remote(src, wide[k].at[owner, r], early_send.at[p, lane], early_recv.at[p, lane], fs=to)

    def act_own(p):
        early_copy(p, 0, f, x_peer).start()
        early_copy(p, 3, f, y_peer).start()
        early_copy(p, 1, f, x_peer).start()
        early_copy(p, 2, f, y_peer).start()

    def act_relay(p):
        early_copy(p, 0, x_peer, x_peer).wait_recv()
        early_copy(p, 4, x_peer, y_peer).start()
        early_copy(p, 3, y_peer, y_peer).wait_recv()
        early_copy(p, 5, y_peer, x_peer).start()

    def early_arrive(p):
        for lane, owner in ((1, x_peer), (2, y_peer), (4, diag), (5, diag)):
            early_copy(p, lane, owner, x_peer).wait_recv()

    for k in heads:
        loads[13 + k].wait()
    for p in range(min(START_PAIRS, len(pairs))):
        act_own(p)

    share.wait()

    def act_join(k):
        own = jnp.dot(fsib[...], basis[k][theirs, :], preferred_element_type=F32)
        parts[pieces_of(k)] += own.reshape(PIECES, piece, rank)

    def hop(j, has_src, has_dst, src_in, snd, lane, to):
        @pl.when((j >= 0) & (j < count))
        def _():
            jj = jnp.clip(j, 0, count - 1)
            copy = remote(snd.at[jj], src_in.at[jj], z_send.at[lane, jj], z_recv.at[lane, jj], tp=to)

            @pl.when(has_src)
            def _():
                copy.wait_recv()

            @pl.when(has_dst)
            def _():
                snd[jj] = (parts[jj] + src_in[jj].astype(F32)).astype(BF16)
                copy.start()

    above = jnp.minimum(t + 2, tp - 2 + c)
    below = jnp.maximum(t - 2, c)

    def z_step(step):
        hop(step - SKEW * z, z > 0, z < zs - 1, up_in, up_snd, 0, above)
        hop(step - SKEW * (zs - 1 - z), z < zs - 1, z > 0, dn_in, dn_snd, 1, below)

    mate_copy = [remote(tot.at[k], sib.at[k], sib_send.at[k], sib_recv.at[k], tp=mate) for k in range(3)]

    def act_total(k):
        for j in range(PIECES):
            i = k * PIECES + j
            whole = parts[i] + up_in[i].astype(F32) + dn_in[i].astype(F32)
            tot[k, j * piece : (j + 1) * piece, :] = whole.astype(BF16)
        mate_copy[k].start()

    def contract(a, b):
        return lax.dot_general(a, b, (((0,), (0,)), ((), ())), preferred_element_type=F32)

    def rows_of(i):
        return pl.ds(pl.multiple_of(i * rb, rb), rb)

    def rs_copy(k, d):
        peer = lax.rem(f + d, n)
        return remote(rs_out[k].at[rows_of(peer)], rs_in[k].at[d - 1], rs_send.at[k, d - 1], rs_recv.at[k, d - 1], fs=peer)

    def ag_copy(k, d, whose):
        peer = lax.rem(f + d, n)
        r = direction[k].at[rows_of(whose)]
        return remote(r, r, ag_send.at[k, d - 1], ag_recv.at[k, d - 1], fs=peer)

    def part_copy(k, d, whose):
        peer = lax.rem(f + d, n)
        r = shares.at[k, whose]
        return remote(r, r, part_send.at[k, d - 1], part_recv.at[k, d - 1], fs=peer)

    def sq_copy(k, d, whose):
        peer = lax.rem(t + d, tp)
        r = sums.at[k, whose]
        return remote(r, r, sq_send.at[k, d - 1], sq_recv.at[k, d - 1], tp=peer)

    def act_project(k):
        loads[4 + k].wait()
        acc = contract(tot[k], cot[k][pl.ds(my_half, half), :])
        mate_copy[k].wait_recv()
        whole = acc + contract(sib[k], cot[k][pl.ds(mate_half, half), :])
        proj[k][...] = whole
        rs_out[k][...] = whole.astype(BF16)
        for d in range(1, n):
            rs_copy(k, d).start()

    def act_moment(k):
        loads[7 + k].wait()
        loads[10 + k].wait()
        r = proj[k][rows_of(f), :]
        for d in range(1, n):
            rs_copy(k, d).wait_recv()
            r = r + rs_in[k][d - 1].astype(F32)
        a = 0.8 * first[k][...] + 0.2 * r
        b = 0.9 * second[k][...] + 0.1 * r * r
        fir[k][...] = a
        sec[k][...] = b
        turned = a / jnp.sqrt(b)
        shares[k, f] = jnp.full((8, 128), jnp.sum(turned * turned), F32)
        direction[k][rows_of(f), :] = turned
        for d in range(1, n):
            part_copy(k, d, f).start()
        for d in range(1, n):
            ag_copy(k, d, f).start()

    def act_tally(k):
        for d in range(1, n):
            part_copy(k, d, lax.rem(f - d + n, n)).wait_recv()
        sums[k, t] = jnp.sum(shares[k], axis=0)
        for d in range(1, tp):
            sq_copy(k, d, t).start()

    rows = pl.ds(pl.multiple_of(f * rows_dev, rows_dev), rows_dev)

    def expand(k, base):
        whole = direction[k][...]
        high = whole.astype(BF16)
        low = (whole - high.astype(F32)).astype(BF16)
        return jnp.dot(
            jnp.concatenate([base, base], axis=1),
            jnp.concatenate([high, low], axis=0),
            preferred_element_type=F32,
        )

    def act_direction(k):
        for d in range(1, n):
            ag_copy(k, d, lax.rem(f - d + n, n)).wait_recv()
        upd[k][...] = expand(k, basis[k][rows, :])

    def scale_of(k):
        total = jnp.sum(sums[k], axis=0)[0:1, 0:1]
        entries = rank * upd[k].shape[1] * tp
        return lax.rsqrt(total / entries + 1e-06)

    late_pairs = [LATE_PAIRS[k] if n == 4 else 1 for k in range(3)]
    hrow = [(rows_dev - early[k]) // (2 * late_pairs[k]) for k in range(3)]

    def block(k, owner, h):
        size = hrow[k]
        return cop[k].at[pl.ds(pl.multiple_of(owner * rows_dev + early[k] + h * size, 8), size)]

    def bulk(k, p, lane, owner, to):
        b = block(k, owner, 2 * p + (lane in (1, 3, 5)))
        i = 6 * p + lane
        return remote(b, b, bulk_send.at[k, i], bulk_recv.at[k, i], fs=to)

    def direct(k, d, h, owner, to):
        b = block(k, owner, h)
        i = 2 * (d - 1) + h
        return remote(b, b, bulk_send.at[k, i], bulk_recv.at[k, i], fs=to)

    def settle(k, at, size, scale):
        own = pl.ds(at, size)
        update = upd[k][own, :] * scale
        upd[k][own, :] = update
        new = master[k][own, :] - 0.05 * update
        mas[k][own, :] = new
        cop[k][pl.ds(pl.multiple_of(f * rows_dev + at, 8), size), :] = new.astype(BF16)

    def act_finish(k):
        if k not in heads:
            loads[13 + k].wait()
        for d in range(1, tp):
            sq_copy(k, d, lax.rem(t - d + tp, tp)).wait_recv()

    def act_send(k, p):
        scale = scale_of(k)
        if n == 4:
            settle(k, early[k] + 2 * p * hrow[k], hrow[k], scale)
            bulk(k, p, 0, f, x_peer).start()
            settle(k, early[k] + (2 * p + 1) * hrow[k], hrow[k], scale)
            bulk(k, p, 3, f, y_peer).start()
            bulk(k, p, 1, f, x_peer).start()
            bulk(k, p, 2, f, y_peer).start()
        else:
            settle(k, 0, rows_dev, scale)
            for d in range(1, n):
                for h in range(2):
                    direct(k, d, h, f, lax.rem(f + d, n)).start()

    def act_forward(k, p):
        bulk(k, p, 0, x_peer, x_peer).wait_recv()
        bulk(k, p, 4, x_peer, y_peer).start()
        bulk(k, p, 3, y_peer, y_peer).wait_recv()
        bulk(k, p, 5, y_peer, x_peer).start()

    def act_local(k):
        for p in range(len(pairs)):
            if pairs[p][0] == k:
                early_arrive(p)
        scale = scale_of(k)
        settle(k, 0, early[k], scale)
        for owner in (x_peer, y_peer, diag):
            r = pl.ds(pl.multiple_of(owner * rows_dev, rows_dev), early[k])
            update = expand(k, basis[k][r, :]) * scale
            new = wide[k][owner] - 0.05 * update
            cop[k][r, :] = new.astype(BF16)

    def act_arrive(k):
        if n == 4:
            for p in range(late_pairs[k]):
                for lane, owner in ((1, x_peer), (2, y_peer), (4, diag), (5, diag)):
                    bulk(k, p, lane, owner, x_peer).wait_recv()
        else:
            for d in range(1, n):
                for h in range(2):
                    owner = lax.rem(f - d + n, n)
                    direct(k, d, h, owner, owner).wait_recv()

    acts = dict(
        join=act_join, relay=act_relay, own=act_own, total=act_total, project=act_project,
        moment=act_moment, tally=act_tally, direction=act_direction, finish=act_finish, send=act_send,
        forward=act_forward, local=act_local, arrive=act_arrive,
    )
    ramp = SKEW * (zs - 1)
    steps = count + ramp
    todo = [(step, 0, z_step, (step,)) for step in range(steps)]
    todo += [(0.5 if k else -1, 1, act_join, (k,)) for k in range(3)]
    if n == 4:
        todo += [(ramp + at, 2, acts[name], args) for at, name, *args in TAIL]
    else:
        for at, name in PLAIN:
            for k in range(3):
                args = (k, 0) if name == "send" else (k,)
                todo.append((ramp + at + k * PIECES, 2, acts[name], args))
    for _, _, act, args in sorted(todo, key=lambda item: item[:2]):
        act(*args)

    for p in range(len(pairs)):
        for lane in range(6):
            early_copy(p, lane, f, x_peer).wait_send()
    for k in range(3):
        mate_copy[k].wait_send()
        for d in range(1, n):
            rs_copy(k, d).wait_send()
            ag_copy(k, d, f).wait_send()
            part_copy(k, d, f).wait_send()
        for d in range(1, tp):
            sq_copy(k, d, t).wait_send()
        if n == 4:
            for p in range(late_pairs[k] if hrow[k] else 0):
                for lane in range(6):
                    bulk(k, p, lane, f, x_peer).wait_send()
        else:
            for d in range(1, n):
                for h in range(2):
                    direct(k, d, h, f, lax.rem(f + d, n)).wait_send()
    for j in range(count):
        @pl.when(z < zs - 1)
        def _():
            remote(up_snd.at[j], up_in.at[j], z_send.at[0, j], z_recv.at[0, j], tp=above).wait_send()

        @pl.when(z > 0)
        def _():
            remote(dn_snd.at[j], dn_in.at[j], z_send.at[1, j], z_recv.at[1, j], tp=below).wait_send()


def emit(*refs):
    copies = [pltpu.make_async_copy(refs[i], refs[15 + i], refs[30].at[i]) for i in range(15)]
    for cp in copies:
        cp.start()
    for cp in copies:
        cp.wait()


def shards(n, tp, *args):
    features = args[0]
    cots, bases, masters, firsts, seconds = (args[1 + i : 16 : 5] for i in range(5))
    tokens, width = features.shape
    rank = bases[0].shape[1]
    rows_dev = masters[0].shape[0]
    whole_rows = rows_dev * n
    half = tokens // 2
    count = 3 * PIECES
    piece = half // PIECES
    cols = [a.shape[1] for a in cots]

    outs = []
    for k in range(3):
        outs += [
            pltpu.VMEM(masters[k].shape, F32),
            pltpu.VMEM(masters[k].shape, F32),
            pltpu.VMEM(firsts[k].shape, F32),
            pltpu.VMEM(firsts[k].shape, F32),
            pltpu.VMEM((whole_rows, cols[k]), BF16),
        ]
    like = lambda arrays: [pltpu.VMEM(a.shape, a.dtype) for a in arrays]
    early, pairs = plan(n, rows_dev)
    lanes = 6 * max(LATE_PAIRS) if n == 4 else 2 * (n - 1)
    dma = lambda *shape: pltpu.SemaphoreType.DMA(shape)
    scratch = (
        [pltpu.VMEM((tokens, width), BF16), pltpu.VMEM((half, width), BF16)]
        + like(cots)
        + like(bases)
        + like(masters)
        + like(firsts)
        + like(seconds)
        + [pltpu.VMEM((count, piece, rank), F32)]
        + [pltpu.VMEM((count, piece, rank), BF16)] * 4
        + [pltpu.VMEM((3, half, rank), BF16)] * 2
        + [pltpu.VMEM((rank, w), F32) for w in cols]
        + [pltpu.VMEM((rank, w), BF16) for w in cols]
        + [pltpu.VMEM((n - 1, rank // n, w), BF16) for w in cols]
        + [pltpu.VMEM((rank, w), F32) for w in cols]
        + [pltpu.VMEM((n, max(e, 16), w), F32) for e, w in zip(early, cols)]
        + [pltpu.VMEM((3, n, 8, 128), F32), pltpu.VMEM((3, tp, 8, 128), F32)]
        + [dma(16), dma(2, count), dma(2, count), dma(4), dma(4)]
        + [dma(3, n - 1)] * 6
        + [dma(3, tp - 1)] * 2
        + [dma(3, lanes)] * 2
        + [dma(max(len(pairs), 1), 6)] * 2
    )
    held = pl.pallas_call(
        functools.partial(kernel, n, tp),
        out_shape=outs,
        in_specs=[pl.BlockSpec(memory_space=pltpu.HBM)] * 16,
        out_specs=[pl.BlockSpec(memory_space=pltpu.VMEM)] * 15,
        scratch_shapes=scratch,
        compiler_params=pltpu.CompilerParams(
            collective_id=0, has_side_effects=True, vmem_limit_bytes=54 * 1024 * 1024
        ),
    )(*args)
    return pl.pallas_call(
        emit,
        out_shape=[jax.ShapeDtypeStruct(a.shape, a.dtype) for a in held],
        in_specs=[pl.BlockSpec(memory_space=pltpu.VMEM)] * 15,
        out_specs=[pl.BlockSpec(memory_space=pltpu.HBM)] * 15,
        scratch_shapes=[pltpu.SemaphoreType.DMA((15,))],
        compiler_params=pltpu.CompilerParams(vmem_limit_bytes=16 * 1024 * 1024),
    )(*held)


def solution(mesh):
    split = P("fs", "tp")
    return jax.shard_map(
        functools.partial(shards, mesh.shape["fs"], mesh.shape["tp"]),
        mesh=mesh,
        in_specs=(split,) + (split, P(), split, split, split) * 3,
        out_specs=(split, split, split, split, P(None, "tp")) * 3,
        check_vma=False,
    )
```

```python
import functools

import jax
import jax.numpy as jnp
from jax import lax
from jax.experimental import pallas as pl
from jax.experimental.pallas import tpu as pltpu
from jax.sharding import PartitionSpec as P

MESH = pl.DeviceIdType.MESH
PIECES = 8
SKEW = 4
SHARES = 4
HEAD = 6
EARLY = (0, 192, 512)
EARLY_ROWS = (16, 16, 64)
LATE_PAIRS = (2, 1, 1)
START_PAIRS = 8
JOINS = (
    (-3, "heads", 0),
    (-2, "open", 0),
    (-0.5, "join", 0, 0, 1),
    (1.5, "join", 0, 1, 2),
    (2.5, "join", 0, 2, 4),
    (3.4, "open", 1),
    (3.5, "join", 1, 0, 4),
    (3.6, "open", 2),
    (3.7, "join", 2, 0, 4),
)
TAIL = (
    (-4, "relay", 0),
    (-4, "relay", 1),
    (-2, "relay", 2),
    (-1.9, "relay", 3),
    (0, "relay", 4),
    (0.1, "own", 8),
    (5, "total", 0, 0),
    (7, "total", 0, 1),
    (7.1, "project", 0, 0),
    (8, "project", 0, 1),
    (8.5, "own", 9),

    (13, "moment", 0),
    (13.05, "relay", 5),
    (13.1, "total", 1, 0),
    (15, "total", 1, 1),
    (15.1, "project", 1, 0),
    (16, "project", 1, 1),
    (17, "tally", 0),
    (17.1, "spread", 0),
    (17.3, "relay", 6),
    (17.4, "relay", 7),
    (17.5, "relay", 8),
    (17.6, "relay", 9),

    (20, "moment", 1),
    (20.1, "direction", 0),
    (21, "finish", 0),
    (21.1, "send", 0, 0),
    (21.2, "total", 2, 0),
    (23, "total", 2, 1),
    (23.1, "project", 2, 0),
    (23.2, "project", 2, 1),
    (23.3, "tally", 1),
    (23.4, "spread", 1),
    (23.5, "send", 0, 1),
    (24, "forward", 0, 0),
    (25, "moment", 2),
    (25.5, "direction", 1),
    (27.6, "finish", 1),
    (28.1, "send", 1, 0),
    (29, "forward", 0, 1),
    (29.5, "tally", 2),
    (29.6, "spread", 2),
    (30, "forward", 1, 0),
    (32, "local", 1),
    (32.1, "direction", 2),
    (32.2, "finish", 2),
    (32.3, "local", 2),
    (32.5, "drain"),
    (33, "arrive", 0),
    (33, "arrive", 1),
)
PLAIN = (
    (5, "total", 0),
    (7, "total", 1),
    (7.1, "project", 0),
    (8, "project", 1),
    (13, "moment"),
    (17, "tally"),
    (21, "direction"),
    (23, "finish"),
    (23.1, "send", 0),
    (60, "arrive"),
)
F32, BF16 = jnp.float32, jnp.bfloat16


def plan(n, rows_dev):
    early = [min(e, rows_dev) if n == 4 else 0 for e in EARLY]
    pairs = []
    for k in (2, 1, 0):
        for at in range(0, early[k], 2 * EARLY_ROWS[k]):
            pairs.append((k, at, EARLY_ROWS[k]))
    return early, pairs


def kernel(n, tp, *refs):
    feat_in = refs[0]
    cot_in, basis_in, master_in, first_in, second_in = (refs[1 + i : 16 : 5] for i in range(5))
    upd, mas, fir, sec, cop = (refs[16 + i : 31 : 5] for i in range(5))
    (feats, fsib, cot, basis, master, first, second, parts, up_in, dn_in, up_snd, dn_snd,
     tot, sib, proj, rs_out, rs_in, direction, wide, shares, sums,
     load_sem, z_send, z_recv, sib_send, sib_recv, rs_send, rs_recv,
     ag_send, ag_recv, part_send, part_recv, sq_send, sq_recv, bulk_send, bulk_recv, early_send, early_recv, early_rest) = (
        refs[31], refs[32], refs[33:36], refs[36:39], refs[39:42], refs[42:45], refs[45:48],
        *refs[48:53], refs[53], refs[54], refs[55:58], refs[58:61], refs[61:64], refs[64:67],
        refs[67:70], refs[70], refs[71], *refs[72:])

    f, t = lax.axis_index("fs"), lax.axis_index("tp")
    zs = tp // 2
    z, c = t // 2, lax.rem(t, 2)
    mate = 2 * z + 1 - c
    half = feats.shape[0] // 2
    width = feats.shape[1]
    rows_dev = master[0].shape[0]
    rank = proj[0].shape[0]
    rb = rank // n
    piece = half // PIECES
    count = 3 * PIECES
    early, pairs = plan(n, rows_dev)

    def remote(src, dst, ssem, rsem, **dev):
        return pltpu.make_async_remote_copy(
            src_ref=src, dst_ref=dst, send_sem=ssem, recv_sem=rsem, device_id=dev, device_id_type=MESH
        )

    def load(src, dst, i):
        cp = pltpu.make_async_copy(src, dst, load_sem.at[i])
        cp.start()
        return cp

    my_half = pl.multiple_of(c * half, half)
    mate_half = pl.multiple_of((1 - c) * half, half)
    loads = [load(feat_in, feats, 0)]
    loads += [load(basis_in[k], basis[k], 1 + k) for k in range(3)]
    heads = [k for k in (2, 1, 0) if early[k]]
    order = heads + [k for k in range(3) if k not in heads]
    grown = {k: load(master_in[k], master[k], 13 + k) for k in heads}
    loads += [load(cot_in[k], cot[k], 4 + k) for k in range(3)]
    loads += [load(first_in[k], first[k], 7 + k) for k in range(3)]
    loads += [load(second_in[k], second[k], 10 + k) for k in range(3)]
    grown.update({k: load(master_in[k], master[k], 13 + k) for k in order if k not in heads})
    loads += [grown[k] for k in range(3)]

    barrier = pltpu.get_barrier_semaphore()
    for d in range(1, n):
        pl.semaphore_signal(barrier, inc=1, device_id={"fs": lax.rem(f + d, n)}, device_id_type=MESH)
    for d in range(1, tp):
        pl.semaphore_signal(barrier, inc=1, device_id={"tp": lax.rem(t + d, tp)}, device_id_type=MESH)

    @pl.when(z == 0)
    def _():
        up_in[...] = jnp.zeros_like(up_in)

    @pl.when(z == zs - 1)
    def _():
        dn_in[...] = jnp.zeros_like(dn_in)

    loads[0].wait()
    pl.semaphore_wait(barrier, n + tp - 2)

    part = half // SHARES

    def share(i):
        src = feats.at[pl.ds(pl.multiple_of(mate_half + i * part, part), part)]
        return remote(src, fsib.at[pl.ds(i * part, part)], sib_send.at[0], sib_recv.at[6 + i], tp=mate)

    for i in range(SHARES):
        share(i).start()

    mine = pl.ds(pl.multiple_of(t * width, width), width)
    theirs = pl.ds(pl.multiple_of(mate * width, width), width)
    x_peer = f + 1 - 2 * lax.rem(f, 2)
    y_peer = lax.rem(f + 2, 4)
    diag = lax.rem(x_peer + 2, 4)

    def early_copy(p, lane, owner, to):
        k, at, size = pairs[p]
        r = pl.ds(at + size * (lane in (1, 3, 5)), size)
        src = master[k].at[r] if lane < 4 else wide[k].at[owner, r]
        rsem = early_recv.at[p, lane // 3] if lane in (0, 3) else early_rest.at[k]
        return remote(src, wide[k].at[owner, r], early_send.at[k], rsem, fs=to)

    def act_own(p):
        early_copy(p, 0, f, x_peer).start()
        early_copy(p, 3, f, y_peer).start()
        early_copy(p, 1, f, x_peer).start()
        early_copy(p, 2, f, y_peer).start()

    def act_relay(p):
        early_copy(p, 0, x_peer, x_peer).wait_recv()
        early_copy(p, 4, x_peer, y_peer).start()
        early_copy(p, 3, y_peer, y_peer).wait_recv()
        early_copy(p, 5, y_peer, x_peer).start()

    def early_all(k, owners):
        r = wide[k].at[pl.ds(0, owners)]
        return remote(r, r, early_send.at[k], early_rest.at[k], fs=x_peer)

    def act_heads(i):
        for k in heads:
            loads[13 + k].wait()
        for p in range(min(START_PAIRS, len(pairs))):
            act_own(p)

    def act_open(k):
        loads[1 + k].wait()
        own = jnp.dot(feats[pl.ds(my_half, half), :], basis[k][mine, :], preferred_element_type=F32)
        parts[pl.ds(k * PIECES, PIECES)] = own.reshape(PIECES, piece, rank)

    def act_join(k, i, to):
        if k == 0:
            for q in range(i, to):
                share(q).wait_recv()
        size = (to - i) * part
        own = jnp.dot(fsib[i * part : i * part + size], basis[k][theirs, :], preferred_element_type=F32)
        at = pl.ds(k * PIECES + i * (PIECES // SHARES), (to - i) * (PIECES // SHARES))
        parts[at] += own.reshape(size // piece, piece, rank)

    def hop(j, has_src, has_dst, src_in, snd, lane, to):
        @pl.when((j >= 0) & (j < count))
        def _():
            jj = jnp.clip(j, 0, count - 1)
            copy = remote(snd.at[jj], src_in.at[jj], z_send.at[lane], z_recv.at[lane, jj], tp=to)

            @pl.when(has_src)
            def _():
                copy.wait_recv()

            @pl.when(has_dst)
            def _():
                snd[jj] = (parts[jj] + src_in[jj].astype(F32)).astype(BF16)
                copy.start()

    above = jnp.minimum(t + 2, tp - 2 + c)
    below = jnp.maximum(t - 2, c)

    def z_step(step):
        hop(step - SKEW * z, z > 0, z < zs - 1, up_in, up_snd, 0, above)
        hop(step - SKEW * (zs - 1 - z), z < zs - 1, z > 0, dn_in, dn_snd, 1, below)

    spans = ((0, HEAD), (HEAD, PIECES))

    def mate_copy(k, p):
        lo, hi = spans[p]
        r = pl.ds(lo * piece, (hi - lo) * piece)
        i = 2 * k + p
        return remote(tot.at[k, r], sib.at[k, r], sib_send.at[1], sib_recv.at[i], tp=mate)

    def act_total(k, p):
        for j in range(*spans[p]):
            i = k * PIECES + j
            whole = parts[i] + up_in[i].astype(F32) + dn_in[i].astype(F32)
            tot[k, j * piece : (j + 1) * piece, :] = whole.astype(BF16)
        mate_copy(k, p).start()

    def contract(a, b):
        return lax.dot_general(a, b, (((0,), (0,)), ((), ())), preferred_element_type=F32)

    def rows_of(i):
        return pl.ds(pl.multiple_of(i * rb, rb), rb)

    def rs_copy(k, d):
        peer = lax.rem(f + d, n)
        return remote(rs_out[k].at[rows_of(peer)], rs_in[k].at[d - 1], rs_send.at[k], rs_recv.at[k], fs=peer)

    def ag_copy(k, d, whose):
        peer = lax.rem(f + d, n)
        r = direction[k].at[rows_of(whose)]
        return remote(r, r, ag_send.at[k], ag_recv.at[k, 0], fs=peer)

    def part_copy(k, d, whose):
        peer = lax.rem(f + d, n)
        r = shares.at[k, whose]
        return remote(r, r, part_send.at[k], part_recv.at[k], fs=peer)

    def sq_copy(k, d, whose):
        peer = lax.rem(t + d, tp)
        r = sums.at[k, whose]
        return remote(r, r, sq_send.at[k], sq_recv.at[k], tp=peer)

    def rs_all(k):
        return remote(rs_in[k], rs_in[k], rs_send.at[k], rs_recv.at[k], fs=lax.rem(f + 1, n))

    def ring_copy(k, lane, owner, to):
        size = rb // 2
        at = pl.multiple_of(owner * rb + size * (lane in (1, 3, 5)), size)
        r = direction[k].at[pl.ds(at, size)]
        i = 1 + lane // 3 if lane in (0, 3) else 0
        return remote(r, r, ag_send.at[k], ag_recv.at[k, i], fs=to)

    def ag_all(k, owners):
        r = direction[k].at[pl.ds(0, owners * rb)]
        return remote(r, r, ag_send.at[k], ag_recv.at[k, 0], fs=lax.rem(f + 1, n))

    def part_all(k):
        r = shares.at[k, pl.ds(0, n - 1)]
        return remote(r, r, part_send.at[k], part_recv.at[k], fs=lax.rem(f + 1, n))

    def sq_all(k):
        r = sums.at[k, pl.ds(0, tp - 1)]
        return remote(r, r, sq_send.at[k], sq_recv.at[k], tp=lax.rem(t + 1, tp))

    def act_project(k, p):
        lo, size = spans[p][0] * piece, (spans[p][1] - spans[p][0]) * piece
        r = pl.ds(lo, size)
        if p == 0:
            loads[4 + k].wait()
        acc = contract(tot[k, r], cot[k][pl.ds(pl.multiple_of(my_half + lo, piece), size), :])
        mate_copy(k, p).wait_recv()
        acc += contract(sib[k, r], cot[k][pl.ds(pl.multiple_of(mate_half + lo, piece), size), :])
        if p == 0:
            proj[k][...] = acc
            return
        whole = proj[k][...] + acc
        proj[k][...] = whole
        rs_out[k][...] = whole.astype(BF16)
        for d in range(1, n):
            rs_copy(k, d).start()

    def act_moment(k):
        loads[7 + k].wait()
        loads[10 + k].wait()
        r = proj[k][rows_of(f), :]
        rs_all(k).wait_recv()
        for d in range(1, n):
            r = r + rs_in[k][d - 1].astype(F32)
        a = 0.8 * first[k][...] + 0.2 * r
        b = 0.9 * second[k][...] + 0.1 * r * r
        fir[k][...] = a
        sec[k][...] = b
        turned = a / jnp.sqrt(b)
        shares[k, f] = jnp.full((8, 128), jnp.sum(turned * turned), F32)
        direction[k][rows_of(f), :] = turned
        for d in range(1, n):
            part_copy(k, d, f).start()
        if n == 4:
            ring_copy(k, 0, f, x_peer).start()
            ring_copy(k, 3, f, y_peer).start()
            ring_copy(k, 1, f, x_peer).start()
            ring_copy(k, 2, f, y_peer).start()
        else:
            for d in range(1, n):
                ag_copy(k, d, f).start()

    def act_spread(k):
        ring_copy(k, 0, x_peer, x_peer).wait_recv()
        ring_copy(k, 4, x_peer, y_peer).start()
        ring_copy(k, 3, y_peer, y_peer).wait_recv()
        ring_copy(k, 5, y_peer, x_peer).start()

    def act_tally(k):
        part_all(k).wait_recv()
        sums[k, t] = jnp.sum(shares[k], axis=0)
        for d in range(1, tp):
            sq_copy(k, d, t).start()

    rows = pl.ds(pl.multiple_of(f * rows_dev, rows_dev), rows_dev)

    def expand(k, base):
        whole = direction[k][...]
        high = whole.astype(BF16)
        low = (whole - high.astype(F32)).astype(BF16)
        return jnp.dot(
            jnp.concatenate([base, base], axis=1),
            jnp.concatenate([high, low], axis=0),
            preferred_element_type=F32,
        )

    def act_direction(k):
        ag_all(k, 2 if n == 4 else n - 1).wait_recv()
        upd[k][...] = expand(k, basis[k][rows, :])

    def scale_of(k):
        total = jnp.sum(sums[k], axis=0)[0:1, 0:1]
        entries = rank * upd[k].shape[1] * tp
        return lax.rsqrt(total / entries + 1e-06)

    late_pairs = [LATE_PAIRS[k] if n == 4 else 1 for k in range(3)]
    hrow = [(rows_dev - early[k]) // (2 * late_pairs[k]) for k in range(3)]

    def block(k, owner, h):
        size = hrow[k]
        return cop[k].at[pl.ds(pl.multiple_of(owner * rows_dev + early[k] + h * size, 8), size)]

    def bulk(k, p, lane, owner, to):
        b = block(k, owner, 2 * p + (lane in (1, 3, 5)))
        i = 2 * p + 1 + lane // 3 if lane in (0, 3) else 0
        return remote(b, b, bulk_send.at[k], bulk_recv.at[k, i], fs=to)

    def bulk_all(k, count):
        r = cop[k].at[pl.ds(0, count)]
        return remote(r, r, bulk_send.at[k], bulk_recv.at[k, 0], fs=lax.rem(f + 1, n))

    def direct(k, d, h, owner, to):
        b = block(k, owner, h)
        return remote(b, b, bulk_send.at[k], bulk_recv.at[k, 0], fs=to)

    def settle(k, at, size, scale):
        own = pl.ds(at, size)
        update = upd[k][own, :] * scale
        upd[k][own, :] = update
        new = master[k][own, :] - 0.05 * update
        mas[k][own, :] = new
        cop[k][pl.ds(pl.multiple_of(f * rows_dev + at, 8), size), :] = new.astype(BF16)

    def act_finish(k):
        if k not in heads:
            loads[13 + k].wait()
        sq_all(k).wait_recv()

    def act_send(k, p):
        scale = scale_of(k)
        if n == 4:
            settle(k, early[k] + 2 * p * hrow[k], hrow[k], scale)
            bulk(k, p, 0, f, x_peer).start()
            settle(k, early[k] + (2 * p + 1) * hrow[k], hrow[k], scale)
            bulk(k, p, 3, f, y_peer).start()
            bulk(k, p, 1, f, x_peer).start()
            bulk(k, p, 2, f, y_peer).start()
        else:
            settle(k, 0, rows_dev, scale)
            for d in range(1, n):
                for h in range(2):
                    direct(k, d, h, f, lax.rem(f + d, n)).start()

    def act_forward(k, p):
        bulk(k, p, 0, x_peer, x_peer).wait_recv()
        bulk(k, p, 4, x_peer, y_peer).start()
        bulk(k, p, 3, y_peer, y_peer).wait_recv()
        bulk(k, p, 5, y_peer, x_peer).start()

    def act_local(k):
        early_all(k, 2).wait_recv()
        scale = scale_of(k)
        settle(k, 0, early[k], scale)
        for owner in (x_peer, y_peer, diag):
            r = pl.ds(pl.multiple_of(owner * rows_dev, rows_dev), early[k])
            update = expand(k, basis[k][r, :]) * scale
            new = wide[k][owner] - 0.05 * update
            cop[k][r, :] = new.astype(BF16)

    def act_arrive(k):
        bulk_all(k, 2 * (rows_dev - early[k]) if n == 4 else (n - 1) * rows_dev).wait_recv()

    def act_drain():
        remote(fsib, fsib, sib_send.at[0], sib_recv.at[0], tp=mate).wait_send()
        remote(tot, sib, sib_send.at[1], sib_recv.at[0], tp=mate).wait_send()
        for k in range(3):
            if early[k]:
                early_all(k, 3).wait_send()
            ag_all(k, n - 1).wait_send()
            for whole in (rs_all, part_all, sq_all):
                whole(k).wait_send()

        @pl.when(z < zs - 1)
        def _():
            remote(up_snd, up_in, z_send.at[0], z_recv.at[0, 0], tp=above).wait_send()

        @pl.when(z > 0)
        def _():
            remote(dn_snd, dn_in, z_send.at[1], z_recv.at[1, 0], tp=below).wait_send()

    acts = dict(
        spread=act_spread,
        heads=act_heads, open=act_open,
        drain=act_drain,
        join=act_join, relay=act_relay, own=act_own, total=act_total, project=act_project,
        moment=act_moment, tally=act_tally, direction=act_direction, finish=act_finish, send=act_send,
        forward=act_forward, local=act_local, arrive=act_arrive,
    )
    ramp = SKEW * (zs - 1)
    steps = count + ramp
    todo = [(step, 0, z_step, (step,)) for step in range(steps)]
    todo += [(at, 1, acts[name], args) for at, name, *args in JOINS]
    if n == 4:
        todo += [(ramp + at, 2, acts[name], args) for at, name, *args in TAIL]
    else:
        for at, name, *extra in PLAIN:
            for k in range(3):
                args = (k, *extra)
                todo.append((ramp + at + k * PIECES, 2, acts[name], args))
    for _, _, act, args in sorted(todo, key=lambda item: item[:2]):
        act(*args)

    if n != 4:
        act_drain()
    for k in range(3):
        if early[k] < rows_dev:
            bulk_all(k, (n - 1) * (rows_dev - early[k])).wait_send()


def emit(*refs):
    copies = [pltpu.make_async_copy(refs[i], refs[15 + i], refs[30].at[i]) for i in range(15)]
    for cp in copies:
        cp.start()
    for cp in copies:
        cp.wait()


def shards(n, tp, *args):
    features = args[0]
    cots, bases, masters, firsts, seconds = (args[1 + i : 16 : 5] for i in range(5))
    tokens, width = features.shape
    rank = bases[0].shape[1]
    rows_dev = masters[0].shape[0]
    whole_rows = rows_dev * n
    half = tokens // 2
    count = 3 * PIECES
    piece = half // PIECES
    cols = [a.shape[1] for a in cots]

    outs = []
    for k in range(3):
        outs += [
            pltpu.VMEM(masters[k].shape, F32),
            pltpu.VMEM(masters[k].shape, F32),
            pltpu.VMEM(firsts[k].shape, F32),
            pltpu.VMEM(firsts[k].shape, F32),
            pltpu.VMEM((whole_rows, cols[k]), BF16),
        ]
    like = lambda arrays: [pltpu.VMEM(a.shape, a.dtype) for a in arrays]
    early, pairs = plan(n, rows_dev)
    dma = lambda *shape: pltpu.SemaphoreType.DMA(shape)
    scratch = (
        [pltpu.VMEM((tokens, width), BF16), pltpu.VMEM((half, width), BF16)]
        + like(cots)
        + like(bases)
        + like(masters)
        + like(firsts)
        + like(seconds)
        + [pltpu.VMEM((count, piece, rank), F32)]
        + [pltpu.VMEM((count, piece, rank), BF16)] * 4
        + [pltpu.VMEM((3, half, rank), BF16)] * 2
        + [pltpu.VMEM((rank, w), F32) for w in cols]
        + [pltpu.VMEM((rank, w), BF16) for w in cols]
        + [pltpu.VMEM((n - 1, rank // n, w), BF16) for w in cols]
        + [pltpu.VMEM((rank, w), F32) for w in cols]
        + [pltpu.VMEM((n, max(e, 16), w), F32) for e, w in zip(early, cols)]
        + [pltpu.VMEM((3, n, 8, 128), F32), pltpu.VMEM((3, tp, 8, 128), F32)]
        + [dma(16), dma(2), dma(2, count), dma(2), dma(6 + SHARES)]
        + [dma(3)] * 3
        + [dma(3, 3)]
        + [dma(3)] * 5
        + [dma(3, 2 * max(LATE_PAIRS) + 1), dma(3), dma(max(len(pairs), 1), 2), dma(3)]
    )
    held = pl.pallas_call(
        functools.partial(kernel, n, tp),
        out_shape=outs,
        in_specs=[pl.BlockSpec(memory_space=pltpu.HBM)] * 16,
        out_specs=[pl.BlockSpec(memory_space=pltpu.VMEM)] * 15,
        scratch_shapes=scratch,
        compiler_params=pltpu.CompilerParams(
            collective_id=0, has_side_effects=True, vmem_limit_bytes=54 * 1024 * 1024
        ),
    )(*args)
    return pl.pallas_call(
        emit,
        out_shape=[jax.ShapeDtypeStruct(a.shape, a.dtype) for a in held],
        in_specs=[pl.BlockSpec(memory_space=pltpu.VMEM)] * 15,
        out_specs=[pl.BlockSpec(memory_space=pltpu.HBM)] * 15,
        scratch_shapes=[pltpu.SemaphoreType.DMA((15,))],
        compiler_params=pltpu.CompilerParams(vmem_limit_bytes=16 * 1024 * 1024),
    )(*held)


def solution(mesh):
    split = P("fs", "tp")
    return jax.shard_map(
        functools.partial(shards, mesh.shape["fs"], mesh.shape["tp"]),
        mesh=mesh,
        in_specs=(split,) + (split, P(), split, split, split) * 3,
        out_specs=(split, split, split, split, P(None, "tp")) * 3,
        check_vma=False,
    )
```

```python
import functools

import jax
import jax.numpy as jnp
from jax import lax
from jax.experimental import pallas as pl
from jax.experimental.pallas import tpu as pltpu
from jax.sharding import PartitionSpec as P

MESH = pl.DeviceIdType.MESH
PIECES = 8
SKEW = 4
SHARES = 4
HEAD = 6
PAIR_ROWS = (64, 64, 256)
BLOCK = 128
SPAN = 120.0
JOINS = (
    (-5, "top", 2),
    (-4, "code", 0, 0),
    (-3, "own", 0),
    (-2, "open", 0),
    (-0.5, "join", 0, 0, 1),
    (1.5, "join", 0, 1, 2),
    (2.5, "join", 0, 2, 4),
    (2.6, "top", 0),
    (2.7, "code", 1, 2),
    (2.8, "own", 1),
    (2.9, "own", 2),
    (3.4, "open", 1),
    (3.5, "join", 1, 0, 4),
    (3.6, "open", 2),
    (3.7, "join", 2, 0, 4),
)
TAIL = (
    (-3.5, "relay", 0),
    (-3, "code", 3, 4),
    (-2.9, "own", 3),
    (-1.9, "relay", 1),
    (-1, "top", 1),
    (0, "relay", 2),
    (0.1, "code", 5, 6),
    (1, "own", 4),
    (5, "total", 0, 0),
    (7, "total", 0, 1),
    (7.1, "project", 0, 0),
    (8, "project", 0, 1),
    (8.5, "relay", 3),
    (9, "own", 5),
    (10, "code", 7, 8),
    (13.1, "total", 1, 0),
    (15, "total", 1, 1),
    (15.1, "project", 1, 0),
    (16, "project", 1, 1),
    (18, "moment", 0),
    (18.1, "relay", 4),
    (21.2, "total", 2, 0),
    (24.0, "total", 2, 1),
    (24.1, "project", 2, 0),
    (24.2, "project", 2, 1),
    (24.3, "moment", 1),
    (24.4, "tally", 0),
    (24.5, "relay", 5),
    (24.6, "spread", 0),
    (24.7, "tally", 1),
    (24.8, "moment", 2),
    (24.9, "own", 6),
    (25.0, "spread", 1),
    (25.1, "tally", 2),
    (25.2, "spread", 2),
    (25.3, "own", 7),
    (25.4, "direction", 0),
    (25.5, "finish", 0),
    (25.6, "settle", 0),
    (25.7, "form", 0, 0),
    (25.8, "relay", 6),
    (25.9, "form", 0, 1),
    (26.0, "form", 0, 2),
    (26.1, "direction", 1),
    (26.2, "direction", 2),
    (26.3, "finish", 1),
    (26.4, "finish", 2),
    (26.5, "own", 8),
    (26.6, "settle", 1),
    (26.7, "settle", 2),
    (26.8, "relay", 7),
    (26.9, "form", 1, 0),
    (27.0, "form", 2, 0),
    (27.1, "form", 2, 1),
    (27.2, "form", 2, 2),
    (27.3, "last", 0, 0),
    (27.4, "relay", 8),
    (27.5, "last", 1, 4),
    (27.6, "form", 1, 1),
    (27.7, "form", 1, 2),
    (27.8, "drain"),
    (27.9, "last", 5, 6),
    (28.0, "last", 7, 8),
)
PLAIN = (
    (5, "total", 0),
    (7, "total", 1),
    (7.1, "project", 0),
    (8, "project", 1),
    (13, "moment"),
    (17, "tally"),
    (21, "direction"),
    (23, "finish"),
    (23.1, "settle"),
    (23.2, "send"),
    (60, "arrive"),
)
F32, BF16 = jnp.float32, jnp.bfloat16


def plan(n, rows_dev):
    pairs = []
    if n == 4:
        for k in (2, 0, 1):
            size = min(PAIR_ROWS[k], rows_dev // 2)
            pairs += [(k, at, size) for at in range(0, rows_dev, 2 * size)]
    return pairs


def kernel(n, tp, *refs):
    feat_in = refs[0]
    cot_in, basis_in, master_in, first_in, second_in = (refs[1 + i : 16 : 5] for i in range(5))
    upd, mas, fir, sec, cop = (refs[16 + i : 31 : 5] for i in range(5))
    (feats, fsib, cot, basis, master, first, second, parts, up_in, dn_in, up_snd, dn_snd,
     tot, sib, proj, rs_out, rs_in, direction, wide, tops, split, shares, sums,
     load_sem, z_send, z_recv, sib_send, sib_recv, rs_send, rs_recv,
     ag_send, ag_recv, part_send, part_recv, sq_send, sq_recv, bulk_send, bulk_recv, early_send, early_recv, early_rest, top_send, top_recv) = (
        refs[31], refs[32], refs[33:36], refs[36:39], refs[39:42], refs[42:45], refs[45:48],
        *refs[48:53], refs[53], refs[54], refs[55:58], refs[58:61], refs[61:64], refs[64:67],
        refs[67:70], refs[70:73], refs[73:76], refs[76], refs[77], *refs[78:])

    f, t = lax.axis_index("fs"), lax.axis_index("tp")
    zs = tp // 2
    z, c = t // 2, lax.rem(t, 2)
    mate = 2 * z + 1 - c
    half = feats.shape[0] // 2
    width = feats.shape[1]
    rows_dev = master[0].shape[0]
    rank = proj[0].shape[0]
    rb = rank // n
    piece = half // PIECES
    count = 3 * PIECES
    pairs = plan(n, rows_dev)
    block_rows = min(BLOCK, rows_dev)

    def remote(src, dst, ssem, rsem, **dev):
        return pltpu.make_async_remote_copy(
            src_ref=src, dst_ref=dst, send_sem=ssem, recv_sem=rsem, device_id=dev, device_id_type=MESH
        )

    def load(src, dst, i):
        cp = pltpu.make_async_copy(src, dst, load_sem.at[i])
        cp.start()
        return cp

    side = lax.rem(c + z, 2)
    my_half = pl.multiple_of(side * half, half)
    mate_half = pl.multiple_of((1 - side) * half, half)
    loads = [load(feat_in, feats, 0)]
    loads += [load(basis_in[k], basis[k], 1 + k) for k in range(3)]
    grown = {2: load(master_in[2], master[2], 15)}
    loads += [load(cot_in[0], cot[0], 4)]
    grown.update({k: load(master_in[k], master[k], 13 + k) for k in (0, 1)})
    loads += [load(cot_in[k], cot[k], 4 + k) for k in (1, 2)]
    loads += [load(first_in[k], first[k], 7 + k) for k in range(3)]
    loads += [load(second_in[k], second[k], 10 + k) for k in range(3)]
    loads += [grown[k] for k in range(3)]

    barrier = pltpu.get_barrier_semaphore()
    for d in range(1, n):
        pl.semaphore_signal(barrier, inc=1, device_id={"fs": lax.rem(f + d, n)}, device_id_type=MESH)
    for d in range(1, tp):
        pl.semaphore_signal(barrier, inc=1, device_id={"tp": lax.rem(t + d, tp)}, device_id_type=MESH)

    @pl.when(z == 0)
    def _():
        up_in[...] = jnp.zeros_like(up_in)

    @pl.when(z == zs - 1)
    def _():
        dn_in[...] = jnp.zeros_like(dn_in)

    loads[0].wait()
    pl.semaphore_wait(barrier, n + tp - 2)

    part = half // SHARES

    def share(i):
        src = feats.at[pl.ds(pl.multiple_of(mate_half + i * part, part), part)]
        return remote(src, fsib.at[pl.ds(i * part, part)], sib_send.at[0], sib_recv.at[6 + i], tp=mate)

    for i in range(SHARES):
        share(i).start()

    mine = pl.ds(pl.multiple_of(t * width, width), width)
    theirs = pl.ds(pl.multiple_of(mate * width, width), width)
    x_peer = f + 1 - 2 * lax.rem(f, 2)
    y_peer = lax.rem(f + 2, 4)
    diag = lax.rem(x_peer + 2, 4)

    def peer_of(d):
        return (diag, x_peer, y_peer)[d - 1] if n == 4 else lax.rem(f + d, n)

    def top_copy(k, d):
        r = tops[k].at[f]
        return remote(r, r, top_send.at[k], top_recv.at[k], fs=peer_of(d))

    def top_all(k):
        r = tops[k].at[pl.ds(0, n - 1)]
        return remote(r, r, top_send.at[k], top_recv.at[k], fs=lax.rem(f + 1, n))

    def act_top(k):
        loads[13 + k].wait()
        tops[k][f] = jnp.maximum(jnp.max(jnp.abs(master[k][...]), axis=0, keepdims=True), 1e-30)
        for d in range(1, n):
            top_copy(k, d).start()

    def act_code(p, to):
        k, at, _ = pairs[p]
        r = slice(at, pairs[to][1] + 2 * pairs[to][2])
        value = master[k][r, :]
        size = jnp.exp2(jnp.abs(value) * (2 * SPAN / tops[k][f]) - SPAN)
        wide[k][f, r, :] = jnp.where(value < 0, -size, size).astype(BF16)

    def early_copy(p, lane, owner, to):
        k, at, size = pairs[p]
        r = wide[k].at[owner, pl.ds(at + size * (lane in (1, 3, 5)), size)]
        if lane in (1, 2):
            rsem = early_rest.at[k]
        else:
            rsem = early_recv.at[p, {0: 0, 3: 1}.get(lane, 2)]
        return remote(r, r, early_send.at[k], rsem, fs=to)

    def act_own(p):
        early_copy(p, 0, f, x_peer).start()
        early_copy(p, 3, f, y_peer).start()
        early_copy(p, 1, f, x_peer).start()
        early_copy(p, 2, f, y_peer).start()

    def act_relay(p):
        early_copy(p, 0, x_peer, x_peer).wait_recv()
        early_copy(p, 4, x_peer, y_peer).start()
        early_copy(p, 3, y_peer, y_peer).wait_recv()
        early_copy(p, 5, y_peer, x_peer).start()

    def early_all(k, sem):
        owners = 3 if sem is None else 1
        r = wide[k].at[pl.ds(0, owners)]
        return remote(r, r, early_send.at[k], early_rest.at[k], fs=x_peer)

    def early_pair(p):
        k, _, size = pairs[p]
        r = wide[k].at[0, pl.ds(0, 2 * size)]
        return remote(r, r, early_send.at[k], early_recv.at[p, 2], fs=x_peer)

    def act_open(k):
        loads[1 + k].wait()
        own = jnp.dot(feats[pl.ds(my_half, half), :], basis[k][mine, :], preferred_element_type=F32)
        parts[pl.ds(k * PIECES, PIECES)] = own.reshape(PIECES, piece, rank)

    def act_join(k, i, to):
        if k == 0:
            for q in range(i, to):
                share(q).wait_recv()
        size = (to - i) * part
        own = jnp.dot(fsib[i * part : i * part + size], basis[k][theirs, :], preferred_element_type=F32)
        at = pl.ds(k * PIECES + i * (PIECES // SHARES), (to - i) * (PIECES // SHARES))
        parts[at] += own.reshape(size // piece, piece, rank)

    def hop(j, has_src, has_dst, src_in, snd, lane, to):
        @pl.when((j >= 0) & (j < count))
        def _():
            jj = jnp.clip(j, 0, count - 1)
            copy = remote(snd.at[jj], src_in.at[jj], z_send.at[lane], z_recv.at[lane, jj], tp=to)

            @pl.when(has_src)
            def _():
                copy.wait_recv()

            @pl.when(has_dst)
            def _():
                snd[jj] = (parts[jj] + src_in[jj].astype(F32)).astype(BF16)
                copy.start()

    above = jnp.where(z < zs - 1, t + 3 - 2 * c, mate)
    below = jnp.where(z > 0, t - 1 - 2 * c, mate)

    def z_step(step):
        hop(step - SKEW * z, z > 0, z < zs - 1, up_in, up_snd, 0, above)
        hop(step - SKEW * (zs - 1 - z), z < zs - 1, z > 0, dn_in, dn_snd, 1, below)

    spans = ((0, HEAD), (HEAD, PIECES))

    def mate_copy(k, p):
        lo, hi = spans[p]
        r = pl.ds(lo * piece, (hi - lo) * piece)
        i = 2 * k + p
        return remote(tot.at[k, r], sib.at[k, r], sib_send.at[1], sib_recv.at[i], tp=mate)

    def act_total(k, p):
        for j in range(*spans[p]):
            i = k * PIECES + j
            whole = parts[i] + up_in[i].astype(F32) + dn_in[i].astype(F32)
            tot[k, j * piece : (j + 1) * piece, :] = whole.astype(BF16)
        mate_copy(k, p).start()

    def contract(a, b):
        return lax.dot_general(a, b, (((0,), (0,)), ((), ())), preferred_element_type=F32)

    def rows_of(i):
        return pl.ds(pl.multiple_of(i * rb, rb), rb)

    def rs_copy(k, d):
        peer = peer_of(d)
        return remote(rs_out[k].at[rows_of(peer)], rs_in[k].at[d - 1], rs_send.at[k], rs_recv.at[k], fs=peer)

    def ag_copy(k, d, whose):
        peer = lax.rem(f + d, n)
        r = direction[k].at[rows_of(whose)]
        return remote(r, r, ag_send.at[k], ag_recv.at[k, 0], fs=peer)

    def part_copy(k, d, whose):
        peer = peer_of(d)
        r = shares.at[k, whose]
        return remote(r, r, part_send.at[k], part_recv.at[k], fs=peer)

    def sq_copy(k, d, whose):
        peer = lax.rem(t + d, tp)
        r = sums.at[k, whose]
        return remote(r, r, sq_send.at[k], sq_recv.at[k], tp=peer)

    def rs_all(k):
        return remote(rs_in[k], rs_in[k], rs_send.at[k], rs_recv.at[k], fs=lax.rem(f + 1, n))

    def ring_copy(k, lane, owner, to):
        size = rb // 2
        at = pl.multiple_of(owner * rb + size * (lane in (1, 3, 5)), size)
        r = direction[k].at[pl.ds(at, size)]
        i = 1 + lane // 3 if lane in (0, 3) else 0
        return remote(r, r, ag_send.at[k], ag_recv.at[k, i], fs=to)

    def ag_all(k, owners):
        r = direction[k].at[pl.ds(0, owners * rb)]
        return remote(r, r, ag_send.at[k], ag_recv.at[k, 0], fs=lax.rem(f + 1, n))

    def part_all(k):
        r = shares.at[k, pl.ds(0, n - 1)]
        return remote(r, r, part_send.at[k], part_recv.at[k], fs=lax.rem(f + 1, n))

    def sq_all(k):
        r = sums.at[k, pl.ds(0, tp - 1)]
        return remote(r, r, sq_send.at[k], sq_recv.at[k], tp=lax.rem(t + 1, tp))

    def act_project(k, p):
        lo, size = spans[p][0] * piece, (spans[p][1] - spans[p][0]) * piece
        r = pl.ds(lo, size)
        if p == 0:
            loads[4 + k].wait()
        acc = contract(tot[k, r], cot[k][pl.ds(pl.multiple_of(my_half + lo, piece), size), :])
        mate_copy(k, p).wait_recv()
        acc += contract(sib[k, r], cot[k][pl.ds(pl.multiple_of(mate_half + lo, piece), size), :])
        if p == 0:
            proj[k][...] = acc
            return
        whole = proj[k][...] + acc
        proj[k][...] = whole
        rs_out[k][...] = whole.astype(BF16)
        for d in range(1, n):
            rs_copy(k, d).start()

    def act_moment(k):
        loads[7 + k].wait()
        loads[10 + k].wait()
        r = proj[k][rows_of(f), :]
        rs_all(k).wait_recv()
        for d in range(1, n):
            r = r + rs_in[k][d - 1].astype(F32)
        a = 0.8 * first[k][...] + 0.2 * r
        b = 0.9 * second[k][...] + 0.1 * r * r
        fir[k][...] = a
        sec[k][...] = b
        turned = a / jnp.sqrt(b)
        shares[k, f] = jnp.full((8, 128), jnp.sum(turned * turned), F32)
        direction[k][rows_of(f), :] = turned
        for d in range(1, n):
            part_copy(k, d, f).start()
        if n == 4:
            ring_copy(k, 0, f, x_peer).start()
            ring_copy(k, 3, f, y_peer).start()
            ring_copy(k, 1, f, x_peer).start()
            ring_copy(k, 2, f, y_peer).start()
        else:
            for d in range(1, n):
                ag_copy(k, d, f).start()

    def act_spread(k):
        ring_copy(k, 0, x_peer, x_peer).wait_recv()
        ring_copy(k, 4, x_peer, y_peer).start()
        ring_copy(k, 3, y_peer, y_peer).wait_recv()
        ring_copy(k, 5, y_peer, x_peer).start()

    def act_tally(k):
        part_all(k).wait_recv()
        sums[k, t] = jnp.sum(shares[k], axis=0)
        for d in range(1, tp):
            sq_copy(k, d, t).start()

    rows = pl.ds(pl.multiple_of(f * rows_dev, rows_dev), rows_dev)

    def expand(k, base):
        return jnp.dot(jnp.concatenate([base, base], axis=1), split[k][...], preferred_element_type=F32)

    def act_direction(k):
        ag_all(k, 2 if n == 4 else n - 1).wait_recv()
        whole = direction[k][...]
        high = whole.astype(BF16)
        split[k][:rank] = high
        split[k][rank:] = (whole - high.astype(F32)).astype(BF16)
        upd[k][...] = expand(k, basis[k][rows, :])

    def scale_of(k):
        total = jnp.sum(sums[k], axis=0)[0:1, 0:1]
        entries = rank * upd[k].shape[1] * tp
        return lax.rsqrt(total / entries + 1e-06)

    def act_finish(k):
        if n != 4:
            loads[13 + k].wait()
        sq_all(k).wait_recv()

    def act_settle(k):
        update = upd[k][...] * scale_of(k)
        upd[k][...] = update
        new = master[k][...] - 0.05 * update
        mas[k][...] = new
        if n != 4:
            cop[k][rows, :] = new.astype(BF16)

    def direct(k, d, owner, to):
        b = cop[k].at[pl.ds(pl.multiple_of(owner * rows_dev, rows_dev), rows_dev)]
        return remote(b, b, bulk_send.at[k], bulk_recv.at[k], fs=to)

    def bulk_all(k):
        r = cop[k].at[pl.ds(0, (n - 1) * rows_dev)]
        return remote(r, r, bulk_send.at[k], bulk_recv.at[k], fs=lax.rem(f + 1, n))

    def act_send(k):
        for d in range(1, n):
            direct(k, d, f, lax.rem(f + d, n)).start()

    def act_arrive(k):
        bulk_all(k).wait_recv()

    def form(k, owner, at, count):
        scale = scale_of(k)
        unit = tops[k][owner] * (0.5 / SPAN)

        def body(i, carry):
            at_i = at + i * block_rows
            r = pl.ds(pl.multiple_of(at_i, block_rows), block_rows)
            g = pl.ds(pl.multiple_of(owner * rows_dev + at_i, block_rows), block_rows)
            update = expand(k, basis[k][g, :]) * scale
            code = wide[k][owner, r, :].astype(F32)
            size = (jnp.log2(jnp.abs(code)) + SPAN) * unit
            cop[k][g, :] = (jnp.where(code < 0, -size, size) - 0.05 * update).astype(BF16)
            return carry

        lax.fori_loop(0, count // block_rows, body, 0)

    def act_form(k, which):
        if which == 0:
            top_all(k).wait_recv()
        if which == 1:
            early_all(k, 0).wait_recv()
        form(k, (f, x_peer, y_peer)[which], 0, rows_dev)

    def act_last(p, to):
        for q in range(p, to + 1):
            early_pair(q).wait_recv()
        k, at, _ = pairs[p]
        form(k, diag, at, pairs[to][1] + 2 * pairs[to][2] - at)

    def act_drain():
        remote(fsib, fsib, sib_send.at[0], sib_recv.at[0], tp=mate).wait_send()
        remote(tot, sib, sib_send.at[1], sib_recv.at[0], tp=mate).wait_send()
        for k in range(3):
            if n == 4:
                early_all(k, None).wait_send()
                top_all(k).wait_send()
            ag_all(k, n - 1).wait_send()
            for whole in (rs_all, part_all, sq_all):
                whole(k).wait_send()

        @pl.when(z < zs - 1)
        def _():
            remote(up_snd, up_in, z_send.at[0], z_recv.at[0, 0], tp=above).wait_send()

        @pl.when(z > 0)
        def _():
            remote(dn_snd, dn_in, z_send.at[1], z_recv.at[1, 0], tp=below).wait_send()

    acts = dict(
        top=act_top, code=act_code, open=act_open, join=act_join, relay=act_relay, own=act_own,
        total=act_total, project=act_project, moment=act_moment, spread=act_spread, tally=act_tally,
        direction=act_direction, finish=act_finish, settle=act_settle, send=act_send,
        form=act_form, last=act_last, arrive=act_arrive, drain=act_drain,
    )
    ramp = SKEW * (zs - 1)
    steps = count + ramp
    todo = [(step, 0, z_step, (step,)) for step in range(steps)]
    todo += [(at, 1, acts[name], args) for at, name, *args in JOINS if n == 4 or name in ("open", "join")]
    if n == 4:
        todo += [(ramp + at, 2, acts[name], args) for at, name, *args in TAIL]
    else:
        for at, name, *extra in PLAIN:
            for k in range(3):
                args = (k, *extra)
                todo.append((ramp + at + k * PIECES, 2, acts[name], args))
    for _, _, act, args in sorted(todo, key=lambda item: item[:2]):
        act(*args)

    if n != 4:
        act_drain()
    for k in range(3):
        if n != 4:
            bulk_all(k).wait_send()


def emit(*refs):
    copies = [pltpu.make_async_copy(refs[i], refs[15 + i], refs[30].at[i]) for i in range(15)]
    for cp in copies:
        cp.start()
    for cp in copies:
        cp.wait()


def shards(n, tp, *args):
    features = args[0]
    cots, bases, masters, firsts, seconds = (args[1 + i : 16 : 5] for i in range(5))
    tokens, width = features.shape
    rank = bases[0].shape[1]
    rows_dev = masters[0].shape[0]
    whole_rows = rows_dev * n
    half = tokens // 2
    count = 3 * PIECES
    piece = half // PIECES
    cols = [a.shape[1] for a in cots]

    outs = []
    for k in range(3):
        outs += [
            pltpu.VMEM(masters[k].shape, F32),
            pltpu.VMEM(masters[k].shape, F32),
            pltpu.VMEM(firsts[k].shape, F32),
            pltpu.VMEM(firsts[k].shape, F32),
            pltpu.VMEM((whole_rows, cols[k]), BF16),
        ]
    like = lambda arrays: [pltpu.VMEM(a.shape, a.dtype) for a in arrays]
    pairs = plan(n, rows_dev)
    wide = (n, rows_dev) if n == 4 else (1, 16)
    dma = lambda *shape: pltpu.SemaphoreType.DMA(shape)
    scratch = (
        [pltpu.VMEM((tokens, width), BF16), pltpu.VMEM((half, width), BF16)]
        + like(cots)
        + like(bases)
        + like(masters)
        + like(firsts)
        + like(seconds)
        + [pltpu.VMEM((count, piece, rank), F32)]
        + [pltpu.VMEM((count, piece, rank), BF16)] * 4
        + [pltpu.VMEM((3, half, rank), BF16)] * 2
        + [pltpu.VMEM((rank, w), F32) for w in cols]
        + [pltpu.VMEM((rank, w), BF16) for w in cols]
        + [pltpu.VMEM((n - 1, rank // n, w), BF16) for w in cols]
        + [pltpu.VMEM((rank, w), F32) for w in cols]
        + [pltpu.VMEM((*wide, w), BF16) for w in cols]
        + [pltpu.VMEM((n, 1, w), F32) for w in cols]
        + [pltpu.VMEM((2 * rank, w), BF16) for w in cols]
        + [pltpu.VMEM((3, n, 8, 128), F32), pltpu.VMEM((3, tp, 8, 128), F32)]
        + [dma(16), dma(2), dma(2, count), dma(2), dma(6 + SHARES)]
        + [dma(3)] * 3
        + [dma(3, 3)]
        + [dma(3)] * 5
        + [dma(3), dma(3), dma(max(len(pairs), 1), 3)] + [dma(3)] * 3
    )
    held = pl.pallas_call(
        functools.partial(kernel, n, tp),
        out_shape=outs,
        in_specs=[pl.BlockSpec(memory_space=pltpu.HBM)] * 16,
        out_specs=[pl.BlockSpec(memory_space=pltpu.VMEM)] * 15,
        scratch_shapes=scratch,
        compiler_params=pltpu.CompilerParams(
            collective_id=0, has_side_effects=True, vmem_limit_bytes=54 * 1024 * 1024
        ),
    )(*args)
    return pl.pallas_call(
        emit,
        out_shape=[jax.ShapeDtypeStruct(a.shape, a.dtype) for a in held],
        in_specs=[pl.BlockSpec(memory_space=pltpu.VMEM)] * 15,
        out_specs=[pl.BlockSpec(memory_space=pltpu.HBM)] * 15,
        scratch_shapes=[pltpu.SemaphoreType.DMA((15,))],
        compiler_params=pltpu.CompilerParams(vmem_limit_bytes=16 * 1024 * 1024),
    )(*held)


def solution(mesh):
    split = P("fs", "tp")
    return jax.shard_map(
        functools.partial(shards, mesh.shape["fs"], mesh.shape["tp"]),
        mesh=mesh,
        in_specs=(split,) + (split, P(), split, split, split) * 3,
        out_specs=(split, split, split, split, P(None, "tp")) * 3,
        check_vma=False,
    )
```

```python
import functools

import jax
import jax.numpy as jnp
from jax import lax
from jax.experimental import pallas as pl
from jax.experimental.pallas import tpu as pltpu
from jax.sharding import PartitionSpec as P

MESH = pl.DeviceIdType.MESH
PIECES = 8
SKEW = 4
SHARES = 4
HEAD = 6
PAIR_ROWS = (64, 64, 256)
BLOCK = 128
SPAN = 120.0
JOINS = (
    (-5, "top", 2),
    (-4, "code", 0, 0),
    (-3, "own", 0),
    (-2, "open", 0),
    (-0.5, "join", 0, 0, 1),
    (1.5, "join", 0, 1, 2),
    (2.5, "join", 0, 2, 4),
    (2.6, "top", 0),
    (2.7, "code", 1, 2),
    (2.8, "own", 1),
    (2.9, "own", 2),
    (3.4, "open", 1),
    (3.5, "join", 1, 0, 4),
    (3.6, "open", 2),
    (3.7, "join", 2, 0, 4),
)
TAIL = (
    (-3.5, "relay", 0),
    (-3, "code", 3, 4),
    (-2.9, "own", 3),
    (-1.9, "relay", 1),
    (-1, "top", 1),
    (0, "relay", 2),
    (0.1, "code", 5, 6),
    (5, "total", 0, 0),
    (7, "total", 0, 1),
    (7.1, "project", 0, 0),
    (8, "project", 0, 1),
    (8.2, "own", 4),
    (8.5, "relay", 3),
    (10, "code", 7, 8),
    (13.1, "total", 1, 0),
    (14.5, "moment", 0),
    (15, "total", 1, 1),
    (15.1, "project", 1, 0),
    (16, "project", 1, 1),
    (16.5, "own", 5),
    (20.5, "tally", 0),
    (20.6, "spread", 0),
    (20.7, "relay", 4),
    (21.2, "total", 2, 0),
    (24.0, "total", 2, 1),
    (24.1, "project", 2, 0),
    (24.2, "project", 2, 1),
    (24.3, "moment", 1),
    (24.4, "relay", 5),
    (24.5, "own", 6),
    (24.6, "direction", 0),
    (24.7, "finish", 0),
    (24.8, "settle", 0),
    (24.9, "form", 0, 0),
    (25.0, "moment", 2),
    (25.1, "tally", 1),
    (25.2, "spread", 1),
    (25.3, "own", 7),
    (25.4, "form", 0, 1),
    (25.5, "tally", 2),
    (25.6, "spread", 2),
    (25.7, "relay", 6),
    (25.8, "own", 8),
    (25.9, "form", 0, 2),
    (26.0, "direction", 1),
    (26.1, "finish", 1),
    (26.2, "settle", 1),
    (26.3, "relay", 7),
    (26.4, "last", 1, 4),
    (26.5, "form", 1, 0),
    (26.6, "direction", 2),
    (26.7, "finish", 2),
    (26.8, "settle", 2),
    (26.9, "form", 2, 0),
    (27.0, "form", 2, 1),
    (27.1, "form", 2, 2),
    (27.2, "relay", 8),
    (27.3, "last", 0, 0),
    (27.4, "form", 1, 1),
    (27.5, "form", 1, 2),
    (27.6, "drain"),
    (27.7, "last", 5, 6),
    (27.8, "last", 7, 8),
)
PLAIN = (
    (5, "total", 0),
    (7, "total", 1),
    (7.1, "project", 0),
    (8, "project", 1),
    (13, "moment"),
    (17, "tally"),
    (21, "direction"),
    (23, "finish"),
    (23.1, "settle"),
    (23.2, "send"),
    (60, "arrive"),
)
F32, BF16 = jnp.float32, jnp.bfloat16


def peak(value):
    return jnp.maximum(jnp.max(jnp.abs(value), axis=0, keepdims=True), 1e-30)


def coded(value, top):
    size = jnp.exp2(jnp.abs(value) * (2 * SPAN / top) - SPAN)
    return jnp.where(value < 0, -size, size).astype(BF16)


def decoded(code, top):
    code = code.astype(F32)
    size = (jnp.log2(jnp.abs(code)) + SPAN) * (top * (0.5 / SPAN))
    return jnp.where(code < 0, -size, size)


def plan(n, rows_dev):
    pairs = []
    if n == 4:
        for k in (2, 0, 1):
            size = min(PAIR_ROWS[k], rows_dev // 2)
            pairs += [(k, at, size) for at in range(0, rows_dev, 2 * size)]
    return pairs


def kernel(n, tp, *refs):
    feat_in = refs[0]
    cot_in, basis_in, master_in, first_in, second_in = (refs[1 + i : 16 : 5] for i in range(5))
    upd, mas, fir, sec, cop = (refs[16 + i : 31 : 5] for i in range(5))
    (feats, fsib, cot, basis, master, first, second, parts, up_in, dn_in, up_snd, dn_snd,
     tot, sib, proj, rs_out, rs_in, direction, wide, tops, split, marks, sums,
     load_sem, z_send, z_recv, sib_send, sib_recv, rs_send, rs_recv,
     ag_send, ag_recv, part_send, part_recv, sq_send, sq_recv, bulk_send, bulk_recv, early_send, early_recv, early_rest, top_send, top_recv) = (
        refs[31], refs[32], refs[33:36], refs[36:39], refs[39:42], refs[42:45], refs[45:48],
        *refs[48:53], refs[53], refs[54], refs[55:58], refs[58:61], refs[61:64], refs[64:67],
        refs[67:70], refs[70:73], refs[73:76], refs[76:79], refs[79], *refs[80:])

    f, t = lax.axis_index("fs"), lax.axis_index("tp")
    zs = tp // 2
    z, c = t // 2, lax.rem(t, 2)
    mate = 2 * z + 1 - c
    half = feats.shape[0] // 2
    width = feats.shape[1]
    rows_dev = master[0].shape[0]
    rank = proj[0].shape[0]
    rb = rank // n
    piece = half // PIECES
    count = 3 * PIECES
    pairs = plan(n, rows_dev)
    block_rows = min(BLOCK, rows_dev)

    def remote(src, dst, ssem, rsem, **dev):
        return pltpu.make_async_remote_copy(
            src_ref=src, dst_ref=dst, send_sem=ssem, recv_sem=rsem, device_id=dev, device_id_type=MESH
        )

    def load(src, dst, i):
        cp = pltpu.make_async_copy(src, dst, load_sem.at[i])
        cp.start()
        return cp

    side = lax.rem(c + z, 2)
    my_half = pl.multiple_of(side * half, half)
    mate_half = pl.multiple_of((1 - side) * half, half)
    loads = [load(feat_in, feats, 0)]
    loads += [load(basis_in[k], basis[k], 1 + k) for k in range(3)]
    grown = {2: load(master_in[2], master[2], 15)}
    loads += [load(cot_in[0], cot[0], 4)]
    grown.update({k: load(master_in[k], master[k], 13 + k) for k in (0, 1)})
    loads += [load(cot_in[k], cot[k], 4 + k) for k in (1, 2)]
    loads += [load(first_in[k], first[k], 7 + k) for k in range(3)]
    loads += [load(second_in[k], second[k], 10 + k) for k in range(3)]
    loads += [grown[k] for k in range(3)]

    barrier = pltpu.get_barrier_semaphore()
    for d in range(1, n):
        pl.semaphore_signal(barrier, inc=1, device_id={"fs": lax.rem(f + d, n)}, device_id_type=MESH)
    for d in range(1, tp):
        pl.semaphore_signal(barrier, inc=1, device_id={"tp": lax.rem(t + d, tp)}, device_id_type=MESH)

    @pl.when(z == 0)
    def _():
        up_in[...] = jnp.zeros_like(up_in)

    @pl.when(z == zs - 1)
    def _():
        dn_in[...] = jnp.zeros_like(dn_in)

    loads[0].wait()
    pl.semaphore_wait(barrier, n + tp - 2)

    part = half // SHARES

    def share(i):
        src = feats.at[pl.ds(pl.multiple_of(mate_half + i * part, part), part)]
        return remote(src, fsib.at[pl.ds(i * part, part)], sib_send.at[0], sib_recv.at[6 + i], tp=mate)

    for i in range(SHARES):
        share(i).start()

    mine = pl.ds(pl.multiple_of(t * width, width), width)
    theirs = pl.ds(pl.multiple_of(mate * width, width), width)
    x_peer = f + 1 - 2 * lax.rem(f, 2)
    y_peer = lax.rem(f + 2, 4)
    diag = lax.rem(x_peer + 2, 4)

    def peer_of(d):
        return (diag, x_peer, y_peer)[d - 1] if n == 4 else lax.rem(f + d, n)

    def top_copy(k, d):
        r = tops[k].at[f]
        return remote(r, r, top_send.at[k], top_recv.at[k], fs=peer_of(d))

    def top_all(k):
        r = tops[k].at[pl.ds(0, n - 1)]
        return remote(r, r, top_send.at[k], top_recv.at[k], fs=lax.rem(f + 1, n))

    def act_top(k):
        loads[13 + k].wait()
        tops[k][f] = peak(master[k][...])
        for d in range(1, n):
            top_copy(k, d).start()

    def act_code(p, to):
        k, at, _ = pairs[p]
        r = slice(at, pairs[to][1] + 2 * pairs[to][2])
        wide[k][f, r, :] = coded(master[k][r, :], tops[k][f])

    def early_copy(p, lane, owner, to):
        k, at, size = pairs[p]
        r = wide[k].at[owner, pl.ds(at + size * (lane in (1, 3, 5)), size)]
        if lane in (1, 2):
            rsem = early_rest.at[k]
        else:
            rsem = early_recv.at[p, {0: 0, 3: 1}.get(lane, 2)]
        return remote(r, r, early_send.at[k], rsem, fs=to)

    def act_own(p):
        early_copy(p, 0, f, x_peer).start()
        early_copy(p, 3, f, y_peer).start()
        early_copy(p, 1, f, x_peer).start()
        early_copy(p, 2, f, y_peer).start()

    def act_relay(p):
        early_copy(p, 0, x_peer, x_peer).wait_recv()
        early_copy(p, 4, x_peer, y_peer).start()
        early_copy(p, 3, y_peer, y_peer).wait_recv()
        early_copy(p, 5, y_peer, x_peer).start()

    def early_all(k, sem):
        owners = 3 if sem is None else 1
        r = wide[k].at[pl.ds(0, owners)]
        return remote(r, r, early_send.at[k], early_rest.at[k], fs=x_peer)

    def early_pair(p):
        k, _, size = pairs[p]
        r = wide[k].at[0, pl.ds(0, 2 * size)]
        return remote(r, r, early_send.at[k], early_recv.at[p, 2], fs=x_peer)

    def act_open(k):
        loads[1 + k].wait()
        own = jnp.dot(feats[pl.ds(my_half, half), :], basis[k][mine, :], preferred_element_type=F32)
        parts[pl.ds(k * PIECES, PIECES)] = own.reshape(PIECES, piece, rank)

    def act_join(k, i, to):
        if k == 0:
            for q in range(i, to):
                share(q).wait_recv()
        size = (to - i) * part
        own = jnp.dot(fsib[i * part : i * part + size], basis[k][theirs, :], preferred_element_type=F32)
        at = pl.ds(k * PIECES + i * (PIECES // SHARES), (to - i) * (PIECES // SHARES))
        parts[at] += own.reshape(size // piece, piece, rank)

    def hop(j, has_src, has_dst, src_in, snd, lane, to):
        @pl.when((j >= 0) & (j < count))
        def _():
            jj = jnp.clip(j, 0, count - 1)
            copy = remote(snd.at[jj], src_in.at[jj], z_send.at[lane], z_recv.at[lane, jj], tp=to)

            @pl.when(has_src)
            def _():
                copy.wait_recv()

            @pl.when(has_dst)
            def _():
                snd[jj] = (parts[jj] + src_in[jj].astype(F32)).astype(BF16)
                copy.start()

    above = jnp.where(z < zs - 1, t + 3 - 2 * c, mate)
    below = jnp.where(z > 0, t - 1 - 2 * c, mate)

    def z_step(step):
        hop(step - SKEW * z, z > 0, z < zs - 1, up_in, up_snd, 0, above)
        hop(step - SKEW * (zs - 1 - z), z < zs - 1, z > 0, dn_in, dn_snd, 1, below)

    spans = ((0, HEAD), (HEAD, PIECES))

    def mate_copy(k, p):
        lo, hi = spans[p]
        r = pl.ds(lo * piece, (hi - lo) * piece)
        i = 2 * k + p
        return remote(tot.at[k, r], sib.at[k, r], sib_send.at[1], sib_recv.at[i], tp=mate)

    def act_total(k, p):
        for j in range(*spans[p]):
            i = k * PIECES + j
            whole = parts[i] + up_in[i].astype(F32) + dn_in[i].astype(F32)
            tot[k, j * piece : (j + 1) * piece, :] = whole.astype(BF16)
        mate_copy(k, p).start()

    def contract(a, b):
        return lax.dot_general(a, b, (((0,), (0,)), ((), ())), preferred_element_type=F32)

    def rows_of(i):
        return pl.ds(pl.multiple_of(i * rb, rb), rb)

    def rs_copy(k, d):
        peer = peer_of(d)
        return remote(rs_out[k].at[rows_of(peer)], rs_in[k].at[d - 1], rs_send.at[k], rs_recv.at[k], fs=peer)

    def ag_copy(k, d, whose):
        peer = lax.rem(f + d, n)
        r = direction[k].at[rows_of(whose)]
        return remote(r, r, ag_send.at[k], ag_recv.at[k, 0], fs=peer)

    def part_copy(k, d, whose):
        peer = peer_of(d)
        r = marks[k].at[whose]
        return remote(r, r, part_send.at[k], part_recv.at[k], fs=peer)

    def sq_copy(k, d, whose):
        peer = lax.rem(t + d, tp)
        r = sums.at[k, whose]
        return remote(r, r, sq_send.at[k], sq_recv.at[k], tp=peer)

    def rs_all(k):
        return remote(rs_in[k], rs_in[k], rs_send.at[k], rs_recv.at[k], fs=lax.rem(f + 1, n))

    def ring_copy(k, lane, owner, to):
        size = rb // 2
        at = pl.multiple_of(owner * rb + size * (lane in (1, 3, 5)), size)
        r = direction[k].at[pl.ds(at, size)]
        i = 1 + lane // 3 if lane in (0, 3) else 0
        return remote(r, r, ag_send.at[k], ag_recv.at[k, i], fs=to)

    def ag_all(k, owners):
        r = direction[k].at[pl.ds(0, owners * rb)]
        return remote(r, r, ag_send.at[k], ag_recv.at[k, 0], fs=lax.rem(f + 1, n))

    def part_all(k):
        r = marks[k].at[pl.ds(0, n - 1)]
        return remote(r, r, part_send.at[k], part_recv.at[k], fs=lax.rem(f + 1, n))

    def sq_all(k):
        r = sums.at[k, pl.ds(0, tp - 1)]
        return remote(r, r, sq_send.at[k], sq_recv.at[k], tp=lax.rem(t + 1, tp))

    def act_project(k, p):
        lo, size = spans[p][0] * piece, (spans[p][1] - spans[p][0]) * piece
        r = pl.ds(lo, size)
        if p == 0:
            loads[4 + k].wait()
        acc = contract(tot[k, r], cot[k][pl.ds(pl.multiple_of(my_half + lo, piece), size), :])
        mate_copy(k, p).wait_recv()
        acc += contract(sib[k, r], cot[k][pl.ds(pl.multiple_of(mate_half + lo, piece), size), :])
        if p == 0:
            proj[k][...] = acc
            return
        whole = proj[k][...] + acc
        proj[k][...] = whole
        rs_out[k][...] = whole.astype(BF16)
        for d in range(1, n):
            rs_copy(k, d).start()

    def act_moment(k):
        loads[7 + k].wait()
        loads[10 + k].wait()
        r = proj[k][rows_of(f), :]
        rs_all(k).wait_recv()
        for d in range(1, n):
            r = r + rs_in[k][d - 1].astype(F32)
        a = 0.8 * first[k][...] + 0.2 * r
        b = 0.9 * second[k][...] + 0.1 * r * r
        fir[k][...] = a
        sec[k][...] = b
        turned = a / jnp.sqrt(b)
        top = peak(turned)
        marks[k][f, :, :128] = jnp.full((1, 128), jnp.sum(turned * turned), F32)
        marks[k][f, :, 128:] = top
        direction[k][rows_of(f), :] = coded(turned, top)
        for d in range(1, n):
            part_copy(k, d, f).start()
        if n == 4:
            ring_copy(k, 0, f, x_peer).start()
            ring_copy(k, 3, f, y_peer).start()
            ring_copy(k, 1, f, x_peer).start()
            ring_copy(k, 2, f, y_peer).start()
        else:
            for d in range(1, n):
                ag_copy(k, d, f).start()

    def act_spread(k):
        ring_copy(k, 0, x_peer, x_peer).wait_recv()
        ring_copy(k, 4, x_peer, y_peer).start()
        ring_copy(k, 3, y_peer, y_peer).wait_recv()
        ring_copy(k, 5, y_peer, x_peer).start()

    def act_tally(k):
        part_all(k).wait_recv()
        sums[k, t] = jnp.broadcast_to(jnp.sum(marks[k][:, :, :128], axis=0), (8, 128))
        for d in range(1, tp):
            sq_copy(k, d, t).start()

    rows = pl.ds(pl.multiple_of(f * rows_dev, rows_dev), rows_dev)

    def expand(k, base):
        return jnp.dot(jnp.concatenate([base, base], axis=1), split[k][...], preferred_element_type=F32)

    def act_direction(k):
        ag_all(k, 2 if n == 4 else n - 1).wait_recv()
        for i in range(n):
            whole = decoded(direction[k][i * rb : (i + 1) * rb], marks[k][i, :, 128:])
            high = whole.astype(BF16)
            split[k][i * rb : (i + 1) * rb] = high
            split[k][rank + i * rb : rank + (i + 1) * rb] = (whole - high.astype(F32)).astype(BF16)
        upd[k][...] = expand(k, basis[k][rows, :])

    def scale_of(k):
        total = jnp.sum(sums[k], axis=0)[0:1, 0:1]
        entries = rank * upd[k].shape[1] * tp
        return lax.rsqrt(total / entries + 1e-06)

    def act_finish(k):
        if n != 4:
            loads[13 + k].wait()
        sq_all(k).wait_recv()

    def act_settle(k):
        update = upd[k][...] * scale_of(k)
        upd[k][...] = update
        new = master[k][...] - 0.05 * update
        mas[k][...] = new
        if n != 4:
            cop[k][rows, :] = new.astype(BF16)

    def direct(k, d, owner, to):
        b = cop[k].at[pl.ds(pl.multiple_of(owner * rows_dev, rows_dev), rows_dev)]
        return remote(b, b, bulk_send.at[k], bulk_recv.at[k], fs=to)

    def bulk_all(k):
        r = cop[k].at[pl.ds(0, (n - 1) * rows_dev)]
        return remote(r, r, bulk_send.at[k], bulk_recv.at[k], fs=lax.rem(f + 1, n))

    def act_send(k):
        for d in range(1, n):
            direct(k, d, f, lax.rem(f + d, n)).start()

    def act_arrive(k):
        bulk_all(k).wait_recv()

    def form(k, owner, at, count):
        scale = scale_of(k)
        top = tops[k][owner]

        def body(i, carry):
            at_i = at + i * block_rows
            r = pl.ds(pl.multiple_of(at_i, block_rows), block_rows)
            g = pl.ds(pl.multiple_of(owner * rows_dev + at_i, block_rows), block_rows)
            update = expand(k, basis[k][g, :]) * scale
            cop[k][g, :] = (decoded(wide[k][owner, r, :], top) - 0.05 * update).astype(BF16)
            return carry

        lax.fori_loop(0, count // block_rows, body, 0)

    def act_form(k, which):
        if which == 0:
            top_all(k).wait_recv()
        if which == 1:
            early_all(k, 0).wait_recv()
        form(k, (f, x_peer, y_peer)[which], 0, rows_dev)

    def act_last(p, to):
        for q in range(p, to + 1):
            early_pair(q).wait_recv()
        k, at, _ = pairs[p]
        form(k, diag, at, pairs[to][1] + 2 * pairs[to][2] - at)

    def act_drain():
        remote(fsib, fsib, sib_send.at[0], sib_recv.at[0], tp=mate).wait_send()
        remote(tot, sib, sib_send.at[1], sib_recv.at[0], tp=mate).wait_send()
        for k in range(3):
            if n == 4:
                early_all(k, None).wait_send()
                top_all(k).wait_send()
            ag_all(k, n - 1).wait_send()
            for whole in (rs_all, part_all, sq_all):
                whole(k).wait_send()

        @pl.when(z < zs - 1)
        def _():
            remote(up_snd, up_in, z_send.at[0], z_recv.at[0, 0], tp=above).wait_send()

        @pl.when(z > 0)
        def _():
            remote(dn_snd, dn_in, z_send.at[1], z_recv.at[1, 0], tp=below).wait_send()

    acts = dict(
        top=act_top, code=act_code, open=act_open, join=act_join, relay=act_relay, own=act_own,
        total=act_total, project=act_project, moment=act_moment, spread=act_spread, tally=act_tally,
        direction=act_direction, finish=act_finish, settle=act_settle, send=act_send,
        form=act_form, last=act_last, arrive=act_arrive, drain=act_drain,
    )
    ramp = SKEW * (zs - 1)
    steps = count + ramp
    todo = [(step, 0, z_step, (step,)) for step in range(steps)]
    todo += [(at, 1, acts[name], args) for at, name, *args in JOINS if n == 4 or name in ("open", "join")]
    if n == 4:
        todo += [(ramp + at, 2, acts[name], args) for at, name, *args in TAIL]
    else:
        for at, name, *extra in PLAIN:
            for k in range(3):
                args = (k, *extra)
                todo.append((ramp + at + k * PIECES, 2, acts[name], args))
    for _, _, act, args in sorted(todo, key=lambda item: item[:2]):
        act(*args)

    if n != 4:
        act_drain()
    for k in range(3):
        if n != 4:
            bulk_all(k).wait_send()


def emit(*refs):
    copies = [pltpu.make_async_copy(refs[i], refs[15 + i], refs[30].at[i]) for i in range(15)]
    for cp in copies:
        cp.start()
    for cp in copies:
        cp.wait()


def shards(n, tp, *args):
    features = args[0]
    cots, bases, masters, firsts, seconds = (args[1 + i : 16 : 5] for i in range(5))
    tokens, width = features.shape
    rank = bases[0].shape[1]
    rows_dev = masters[0].shape[0]
    whole_rows = rows_dev * n
    half = tokens // 2
    count = 3 * PIECES
    piece = half // PIECES
    cols = [a.shape[1] for a in cots]

    outs = []
    for k in range(3):
        outs += [
            pltpu.VMEM(masters[k].shape, F32),
            pltpu.VMEM(masters[k].shape, F32),
            pltpu.VMEM(firsts[k].shape, F32),
            pltpu.VMEM(firsts[k].shape, F32),
            pltpu.VMEM((whole_rows, cols[k]), BF16),
        ]
    like = lambda arrays: [pltpu.VMEM(a.shape, a.dtype) for a in arrays]
    pairs = plan(n, rows_dev)
    wide = (n, rows_dev) if n == 4 else (1, 16)
    dma = lambda *shape: pltpu.SemaphoreType.DMA(shape)
    scratch = (
        [pltpu.VMEM((tokens, width), BF16), pltpu.VMEM((half, width), BF16)]
        + like(cots)
        + like(bases)
        + like(masters)
        + like(firsts)
        + like(seconds)
        + [pltpu.VMEM((count, piece, rank), F32)]
        + [pltpu.VMEM((count, piece, rank), BF16)] * 4
        + [pltpu.VMEM((3, half, rank), BF16)] * 2
        + [pltpu.VMEM((rank, w), F32) for w in cols]
        + [pltpu.VMEM((rank, w), BF16) for w in cols]
        + [pltpu.VMEM((n - 1, rank // n, w), BF16) for w in cols]
        + [pltpu.VMEM((rank, w), BF16) for w in cols]
        + [pltpu.VMEM((*wide, w), BF16) for w in cols]
        + [pltpu.VMEM((n, 1, w), F32) for w in cols]
        + [pltpu.VMEM((2 * rank, w), BF16) for w in cols]
        + [pltpu.VMEM((n, 1, 128 + w), F32) for w in cols]
        + [pltpu.VMEM((3, tp, 8, 128), F32)]
        + [dma(16), dma(2), dma(2, count), dma(2), dma(6 + SHARES)]
        + [dma(3)] * 3
        + [dma(3, 3)]
        + [dma(3)] * 5
        + [dma(3), dma(3), dma(max(len(pairs), 1), 3)] + [dma(3)] * 3
    )
    held = pl.pallas_call(
        functools.partial(kernel, n, tp),
        out_shape=outs,
        in_specs=[pl.BlockSpec(memory_space=pltpu.HBM)] * 16,
        out_specs=[pl.BlockSpec(memory_space=pltpu.VMEM)] * 15,
        scratch_shapes=scratch,
        compiler_params=pltpu.CompilerParams(
            collective_id=0, has_side_effects=True, vmem_limit_bytes=54 * 1024 * 1024
        ),
    )(*args)
    return pl.pallas_call(
        emit,
        out_shape=[jax.ShapeDtypeStruct(a.shape, a.dtype) for a in held],
        in_specs=[pl.BlockSpec(memory_space=pltpu.VMEM)] * 15,
        out_specs=[pl.BlockSpec(memory_space=pltpu.HBM)] * 15,
        scratch_shapes=[pltpu.SemaphoreType.DMA((15,))],
        compiler_params=pltpu.CompilerParams(vmem_limit_bytes=16 * 1024 * 1024),
    )(*held)


def solution(mesh):
    split = P("fs", "tp")
    return jax.shard_map(
        functools.partial(shards, mesh.shape["fs"], mesh.shape["tp"]),
        mesh=mesh,
        in_specs=(split,) + (split, P(), split, split, split) * 3,
        out_specs=(split, split, split, split, P(None, "tp")) * 3,
        check_vma=False,
    )
```

```python
import functools

import jax
import jax.numpy as jnp
from jax import lax
from jax.experimental import pallas as pl
from jax.experimental.pallas import tpu as pltpu
from jax.sharding import PartitionSpec as P

MESH = pl.DeviceIdType.MESH
PIECES = 8
SKEW = 4
SHARES = 4
HEAD = 6
PAIR_ROWS = (64, 64, 256)
BLOCK = 128
SPAN = 120.0
JOINS = (
    (-5, "top", 2),
    (-4, "code", 0, 0),
    (-3, "own", 0),
    (-2.5, "share"),
    (-2, "open", 0),
    (-0.5, "join", 0, 0, 1),
    (1.5, "join", 0, 1, 2),
    (2.5, "join", 0, 2, 4),
    (2.6, "top", 0),
    (2.7, "code", 1, 2),
    (2.8, "own", 1),
    (2.9, "own", 2),
    (3.4, "open", 1),
    (3.5, "join", 1, 0, 4),
    (3.6, "open", 2),
    (3.7, "join", 2, 0, 4),
)
TAIL = (
    (-3.5, "relay", 0),
    (-3, "code", 3, 4),
    (-2.9, "own", 3),
    (-1.9, "relay", 1),
    (-1, "top", 1),
    (0, "relay", 2),
    (0.1, "code", 5, 6),
    (5, "total", 0, 0),
    (7, "total", 0, 1),
    (7.1, "project", 0, 0),
    (8, "project", 0, 1),
    (8.2, "own", 4),
    (8.5, "relay", 3),
    (10, "code", 7, 8),
    (13.1, "total", 1, 0),
    (14.5, "moment", 0),
    (15, "total", 1, 1),
    (15.1, "project", 1, 0),
    (16, "project", 1, 1),
    (16.5, "own", 5),
    (20.5, "tally", 0),
    (20.6, "spread", 0),
    (20.7, "relay", 4),
    (21.2, "total", 2, 0),
    (24.0, "total", 2, 1),
    (24.1, "project", 2, 0),
    (24.2, "project", 2, 1),
    (24.3, "moment", 1),
    (24.4, "relay", 5),
    (24.5, "own", 6, 0),
    (24.6, "direction", 0),
    (24.7, "finish", 0),
    (24.8, "settle", 0),
    (24.9, "form", 0, 0),
    (25.0, "moment", 2),
    (25.1, "tally", 1),
    (25.2, "spread", 1),
    (25.3, "own", 6, 1),
    (25.4, "own", 7, 0),
    (25.5, "form", 0, 1),
    (25.6, "form", 0, 2),
    (25.7, "last", 1, 4),
    (25.8, "tally", 2),
    (25.9, "spread", 2),
    (26.0, "own", 7, 1),
    (26.1, "relay", 6),
    (26.2, "own", 8, 0),
    (26.3, "direction", 1),
    (26.4, "finish", 1),
    (26.5, "settle", 1),
    (26.6, "form", 1, 0),
    (26.7, "own", 8, 1),
    (26.8, "relay", 7),
    (26.9, "direction", 2),
    (27.0, "finish", 2),
    (27.1, "settle", 2),
    (27.2, "form", 2, 0),
    (27.3, "form", 2, 1),
    (27.4, "relay", 8),
    (27.5, "form", 2, 2),
    (27.6, "last", 0, 0),
    (27.7, "form", 1, 1),
    (27.8, "form", 1, 2),
    (27.9, "drain"),
    (28.0, "last", 5, 6),
    (28.1, "last", 7, 7),
    (99, "last", 8, 8),
)
PLAIN = (
    (5, "total", 0),
    (7, "total", 1),
    (7.1, "project", 0),
    (8, "project", 1),
    (13, "moment"),
    (17, "tally"),
    (21, "direction"),
    (23, "finish"),
    (23.1, "settle"),
    (23.2, "send"),
    (60, "arrive"),
)
F32, BF16 = jnp.float32, jnp.bfloat16


def peak(value):
    return jnp.maximum(jnp.max(jnp.abs(value), axis=0, keepdims=True), 1e-30)


def coded(value, top):
    size = jnp.exp2(jnp.abs(value) * (2 * SPAN / top) - SPAN)
    return jnp.where(value < 0, -size, size).astype(BF16)


def decoded(code, top):
    code = code.astype(F32)
    size = (jnp.log2(jnp.abs(code)) + SPAN) * (top * (0.5 / SPAN))
    return jnp.where(code < 0, -size, size)


def plan(n, rows_dev):
    pairs = []
    if n == 4:
        for k in (2, 0, 1):
            size = min(PAIR_ROWS[k], rows_dev // 2)
            pairs += [(k, at, size) for at in range(0, rows_dev, 2 * size)]
    return pairs


def kernel(n, tp, *refs):
    feat_in = refs[0]
    cot_in, basis_in, master_in, first_in, second_in = (refs[1 + i : 16 : 5] for i in range(5))
    upd, mas, fir, sec, cop = (refs[16 + i : 31 : 5] for i in range(5))
    (feats, fsib, cot, basis, master, first, second, parts, up_in, dn_in, up_snd, dn_snd,
     tot, sib, proj, rs_out, rs_in, direction, wide, tops, split, marks, sums,
     load_sem, z_send, z_recv, sib_send, sib_recv, rs_send, rs_recv,
     ag_send, ag_recv, part_send, part_recv, sq_send, sq_recv, bulk_send, bulk_recv, early_send, early_recv, early_rest, top_send, top_recv) = (
        refs[31], refs[32], refs[33:36], refs[36:39], refs[39:42], refs[42:45], refs[45:48],
        *refs[48:53], refs[53], refs[54], refs[55:58], refs[58:61], refs[61:64], refs[64:67],
        refs[67:70], refs[70:73], refs[73:76], refs[76:79], refs[79], *refs[80:])

    f, t = lax.axis_index("fs"), lax.axis_index("tp")
    zs = tp // 2
    z, c = t // 2, lax.rem(t, 2)
    mate = 2 * z + 1 - c
    half = feats.shape[0] // 2
    width = feats.shape[1]
    rows_dev = master[0].shape[0]
    rank = proj[0].shape[0]
    rb = rank // n
    piece = half // PIECES
    count = 3 * PIECES
    pairs = plan(n, rows_dev)
    block_rows = min(BLOCK, rows_dev)

    def remote(src, dst, ssem, rsem, **dev):
        return pltpu.make_async_remote_copy(
            src_ref=src, dst_ref=dst, send_sem=ssem, recv_sem=rsem, device_id=dev, device_id_type=MESH
        )

    def load(src, dst, i):
        cp = pltpu.make_async_copy(src, dst, load_sem.at[i])
        cp.start()
        return cp

    side = lax.rem(c + z, 2)
    my_half = pl.multiple_of(side * half, half)
    mate_half = pl.multiple_of((1 - side) * half, half)
    grown = {2: load(master_in[2], master[2], 15)}
    loads = [load(feat_in, feats, 0)]
    loads += [load(basis_in[k], basis[k], 1 + k) for k in range(3)]
    loads += [load(cot_in[0], cot[0], 4)]
    grown.update({k: load(master_in[k], master[k], 13 + k) for k in (0, 1)})
    loads += [load(cot_in[k], cot[k], 4 + k) for k in (1, 2)]
    loads += [load(first_in[k], first[k], 7 + k) for k in range(3)]
    loads += [load(second_in[k], second[k], 10 + k) for k in range(3)]
    loads += [grown[k] for k in range(3)]

    barrier = pltpu.get_barrier_semaphore()
    for d in range(1, n):
        pl.semaphore_signal(barrier, inc=1, device_id={"fs": lax.rem(f + d, n)}, device_id_type=MESH)
    for d in range(1, tp):
        pl.semaphore_signal(barrier, inc=1, device_id={"tp": lax.rem(t + d, tp)}, device_id_type=MESH)

    @pl.when(z == 0)
    def _():
        up_in[...] = jnp.zeros_like(up_in)

    @pl.when(z == zs - 1)
    def _():
        dn_in[...] = jnp.zeros_like(dn_in)

    pl.semaphore_wait(barrier, n + tp - 2)

    part = half // SHARES

    def share(i):
        src = feats.at[pl.ds(pl.multiple_of(mate_half + i * part, part), part)]
        return remote(src, fsib.at[pl.ds(i * part, part)], sib_send.at[0], sib_recv.at[6 + i], tp=mate)

    def act_share():
        loads[0].wait()
        for i in range(SHARES):
            share(i).start()

    mine = pl.ds(pl.multiple_of(t * width, width), width)
    theirs = pl.ds(pl.multiple_of(mate * width, width), width)
    x_peer = f + 1 - 2 * lax.rem(f, 2)
    y_peer = lax.rem(f + 2, 4)
    diag = lax.rem(x_peer + 2, 4)

    def peer_of(d):
        return (diag, x_peer, y_peer)[d - 1] if n == 4 else lax.rem(f + d, n)

    def top_copy(k, d):
        r = tops[k].at[f]
        return remote(r, r, top_send.at[k], top_recv.at[k], fs=peer_of(d))

    def top_all(k):
        r = tops[k].at[pl.ds(0, n - 1)]
        return remote(r, r, top_send.at[k], top_recv.at[k], fs=lax.rem(f + 1, n))

    def act_top(k):
        loads[13 + k].wait()
        tops[k][f] = peak(master[k][...])
        for d in range(1, n):
            top_copy(k, d).start()

    def act_code(p, to):
        k, at, _ = pairs[p]
        r = slice(at, pairs[to][1] + 2 * pairs[to][2])
        wide[k][f, r, :] = coded(master[k][r, :], tops[k][f])

    def early_copy(p, lane, owner, to):
        k, at, size = pairs[p]
        r = wide[k].at[owner, pl.ds(at + size * (lane in (1, 3, 5)), size)]
        if lane in (1, 2):
            rsem = early_rest.at[k]
        else:
            rsem = early_recv.at[p, lane // 4]
        return remote(r, r, early_send.at[k], rsem, fs=to)

    def act_own(p, *halves):
        if 0 in (halves or (0,)):
            early_copy(p, 0, f, x_peer).start()
            early_copy(p, 3, f, y_peer).start()
        if 1 in (halves or (1,)):
            early_copy(p, 1, f, x_peer).start()
            early_copy(p, 2, f, y_peer).start()

    def act_relay(p):
        early_pair(p, 0).wait_recv()
        early_copy(p, 4, x_peer, y_peer).start()
        early_copy(p, 5, y_peer, x_peer).start()

    def early_all(k, sem):
        owners = 3 if sem is None else 1
        r = wide[k].at[pl.ds(0, owners)]
        return remote(r, r, early_send.at[k], early_rest.at[k], fs=x_peer)

    def early_pair(p, i):
        k, _, size = pairs[p]
        r = wide[k].at[0, pl.ds(0, 2 * size)]
        return remote(r, r, early_send.at[k], early_recv.at[p, i], fs=x_peer)

    def act_open(k):
        loads[1 + k].wait()
        own = jnp.dot(feats[pl.ds(my_half, half), :], basis[k][mine, :], preferred_element_type=F32)
        parts[pl.ds(k * PIECES, PIECES)] = own.reshape(PIECES, piece, rank)

    def act_join(k, i, to):
        if k == 0:
            for q in range(i, to):
                share(q).wait_recv()
        size = (to - i) * part
        own = jnp.dot(fsib[i * part : i * part + size], basis[k][theirs, :], preferred_element_type=F32)
        at = pl.ds(k * PIECES + i * (PIECES // SHARES), (to - i) * (PIECES // SHARES))
        parts[at] += own.reshape(size // piece, piece, rank)

    def hop(j, has_src, has_dst, src_in, snd, lane, to):
        @pl.when((j >= 0) & (j < count))
        def _():
            jj = jnp.clip(j, 0, count - 1)
            copy = remote(snd.at[jj], src_in.at[jj], z_send.at[lane], z_recv.at[lane, jj], tp=to)

            @pl.when(has_src)
            def _():
                copy.wait_recv()

            @pl.when(has_dst)
            def _():
                snd[jj] = (parts[jj] + src_in[jj].astype(F32)).astype(BF16)
                copy.start()

    above = jnp.where(z < zs - 1, t + 3 - 2 * c, mate)
    below = jnp.where(z > 0, t - 1 - 2 * c, mate)

    def z_step(step):
        hop(step - SKEW * z, z > 0, z < zs - 1, up_in, up_snd, 0, above)
        hop(step - SKEW * (zs - 1 - z), z < zs - 1, z > 0, dn_in, dn_snd, 1, below)

    spans = ((0, HEAD), (HEAD, PIECES))

    def mate_copy(k, p):
        lo, hi = spans[p]
        r = pl.ds(lo * piece, (hi - lo) * piece)
        i = 2 * k + p
        return remote(tot.at[k, r], sib.at[k, r], sib_send.at[1], sib_recv.at[i], tp=mate)

    def act_total(k, p):
        for j in range(*spans[p]):
            i = k * PIECES + j
            whole = parts[i] + up_in[i].astype(F32) + dn_in[i].astype(F32)
            tot[k, j * piece : (j + 1) * piece, :] = whole.astype(BF16)
        mate_copy(k, p).start()

    def contract(a, b):
        return lax.dot_general(a, b, (((0,), (0,)), ((), ())), preferred_element_type=F32)

    def rows_of(i):
        return pl.ds(pl.multiple_of(i * rb, rb), rb)

    def rs_copy(k, d):
        peer = peer_of(d)
        return remote(rs_out[k].at[rows_of(peer)], rs_in[k].at[d - 1], rs_send.at[k], rs_recv.at[k], fs=peer)

    def ag_copy(k, d, whose):
        peer = lax.rem(f + d, n)
        r = direction[k].at[rows_of(whose)]
        return remote(r, r, ag_send.at[k], ag_recv.at[k, 0], fs=peer)

    def part_copy(k, d, whose):
        peer = peer_of(d)
        r = marks[k].at[whose]
        return remote(r, r, part_send.at[k], part_recv.at[k], fs=peer)

    def sq_copy(k, d, whose):
        peer = lax.rem(t + d, tp)
        r = sums.at[k, whose]
        return remote(r, r, sq_send.at[k], sq_recv.at[k], tp=peer)

    def rs_all(k):
        return remote(rs_in[k], rs_in[k], rs_send.at[k], rs_recv.at[k], fs=lax.rem(f + 1, n))

    def ring_copy(k, lane, owner, to):
        size = rb // 2
        at = pl.multiple_of(owner * rb + size * (lane in (1, 3, 5)), size)
        r = direction[k].at[pl.ds(at, size)]
        i = 1 + lane // 3 if lane in (0, 3) else 0
        return remote(r, r, ag_send.at[k], ag_recv.at[k, i], fs=to)

    def ag_all(k, owners):
        r = direction[k].at[pl.ds(0, owners * rb)]
        return remote(r, r, ag_send.at[k], ag_recv.at[k, 0], fs=lax.rem(f + 1, n))

    def part_all(k):
        r = marks[k].at[pl.ds(0, n - 1)]
        return remote(r, r, part_send.at[k], part_recv.at[k], fs=lax.rem(f + 1, n))

    def sq_all(k):
        r = sums.at[k, pl.ds(0, tp - 1)]
        return remote(r, r, sq_send.at[k], sq_recv.at[k], tp=lax.rem(t + 1, tp))

    def act_project(k, p):
        lo, size = spans[p][0] * piece, (spans[p][1] - spans[p][0]) * piece
        r = pl.ds(lo, size)
        if p == 0:
            loads[4 + k].wait()
        acc = contract(tot[k, r], cot[k][pl.ds(pl.multiple_of(my_half + lo, piece), size), :])
        mate_copy(k, p).wait_recv()
        acc += contract(sib[k, r], cot[k][pl.ds(pl.multiple_of(mate_half + lo, piece), size), :])
        if p == 0:
            proj[k][...] = acc
            return
        whole = proj[k][...] + acc
        proj[k][...] = whole
        rs_out[k][...] = whole.astype(BF16)
        for d in range(1, n):
            rs_copy(k, d).start()

    def act_moment(k):
        loads[7 + k].wait()
        loads[10 + k].wait()
        r = proj[k][rows_of(f), :]
        rs_all(k).wait_recv()
        for d in range(1, n):
            r = r + rs_in[k][d - 1].astype(F32)
        a = 0.8 * first[k][...] + 0.2 * r
        b = 0.9 * second[k][...] + 0.1 * r * r
        fir[k][...] = a
        sec[k][...] = b
        turned = a / jnp.sqrt(b)
        top = peak(turned)
        marks[k][f, :, :128] = jnp.full((1, 128), jnp.sum(turned * turned), F32)
        marks[k][f, :, 128:] = top
        direction[k][rows_of(f), :] = coded(turned, top)
        for d in range(1, n):
            part_copy(k, d, f).start()
        if n == 4:
            ring_copy(k, 0, f, x_peer).start()
            ring_copy(k, 3, f, y_peer).start()
            ring_copy(k, 1, f, x_peer).start()
            ring_copy(k, 2, f, y_peer).start()
        else:
            for d in range(1, n):
                ag_copy(k, d, f).start()

    def act_spread(k):
        ring_copy(k, 0, x_peer, x_peer).wait_recv()
        ring_copy(k, 4, x_peer, y_peer).start()
        ring_copy(k, 3, y_peer, y_peer).wait_recv()
        ring_copy(k, 5, y_peer, x_peer).start()

    def act_tally(k):
        part_all(k).wait_recv()
        sums[k, t] = jnp.broadcast_to(jnp.sum(marks[k][:, :, :128], axis=0), (8, 128))
        for d in range(1, tp):
            sq_copy(k, d, t).start()

    rows = pl.ds(pl.multiple_of(f * rows_dev, rows_dev), rows_dev)

    def expand(k, base):
        return jnp.dot(jnp.concatenate([base, base], axis=1), split[k][...], preferred_element_type=F32)

    def act_direction(k):
        ag_all(k, 2 if n == 4 else n - 1).wait_recv()
        for i in range(n):
            whole = decoded(direction[k][i * rb : (i + 1) * rb], marks[k][i, :, 128:])
            high = whole.astype(BF16)
            split[k][i * rb : (i + 1) * rb] = high
            split[k][rank + i * rb : rank + (i + 1) * rb] = (whole - high.astype(F32)).astype(BF16)
        upd[k][...] = expand(k, basis[k][rows, :])

    def scale_of(k):
        total = jnp.sum(sums[k], axis=0)[0:1, 0:1]
        entries = rank * upd[k].shape[1] * tp
        return lax.rsqrt(total / entries + 1e-06)

    def act_finish(k):
        if n != 4:
            loads[13 + k].wait()
        sq_all(k).wait_recv()

    def act_settle(k):
        update = upd[k][...] * scale_of(k)
        upd[k][...] = update
        new = master[k][...] - 0.05 * update
        mas[k][...] = new
        if n != 4:
            cop[k][rows, :] = new.astype(BF16)

    def direct(k, d, owner, to):
        b = cop[k].at[pl.ds(pl.multiple_of(owner * rows_dev, rows_dev), rows_dev)]
        return remote(b, b, bulk_send.at[k], bulk_recv.at[k], fs=to)

    def bulk_all(k):
        r = cop[k].at[pl.ds(0, (n - 1) * rows_dev)]
        return remote(r, r, bulk_send.at[k], bulk_recv.at[k], fs=lax.rem(f + 1, n))

    def act_send(k):
        for d in range(1, n):
            direct(k, d, f, lax.rem(f + d, n)).start()

    def act_arrive(k):
        bulk_all(k).wait_recv()

    def form(k, owner, at, count):
        scale = scale_of(k)
        top = tops[k][owner]

        def body(i, carry):
            at_i = at + i * block_rows
            r = pl.ds(pl.multiple_of(at_i, block_rows), block_rows)
            g = pl.ds(pl.multiple_of(owner * rows_dev + at_i, block_rows), block_rows)
            update = expand(k, basis[k][g, :]) * scale
            cop[k][g, :] = (decoded(wide[k][owner, r, :], top) - 0.05 * update).astype(BF16)
            return carry

        lax.fori_loop(0, count // block_rows, body, 0)

    def act_form(k, which):
        if which == 0:
            top_all(k).wait_recv()
        if which == 1:
            early_all(k, 0).wait_recv()
        form(k, (f, x_peer, y_peer)[which], 0, rows_dev)

    def act_last(p, to):
        for q in range(p, to + 1):
            early_pair(q, 1).wait_recv()
        k, at, _ = pairs[p]
        form(k, diag, at, pairs[to][1] + 2 * pairs[to][2] - at)

    def act_drain():
        remote(fsib, fsib, sib_send.at[0], sib_recv.at[0], tp=mate).wait_send()
        remote(tot, sib, sib_send.at[1], sib_recv.at[0], tp=mate).wait_send()
        for k in range(3):
            if n == 4:
                early_all(k, None).wait_send()
                top_all(k).wait_send()
            ag_all(k, n - 1).wait_send()
            for whole in (rs_all, part_all, sq_all):
                whole(k).wait_send()

        @pl.when(z < zs - 1)
        def _():
            remote(up_snd, up_in, z_send.at[0], z_recv.at[0, 0], tp=above).wait_send()

        @pl.when(z > 0)
        def _():
            remote(dn_snd, dn_in, z_send.at[1], z_recv.at[1, 0], tp=below).wait_send()

    acts = dict(
        top=act_top, code=act_code, open=act_open, join=act_join, relay=act_relay, own=act_own,
        total=act_total, project=act_project, moment=act_moment, spread=act_spread, tally=act_tally,
        direction=act_direction, finish=act_finish, settle=act_settle, send=act_send,
        form=act_form, share=act_share, last=act_last, arrive=act_arrive, drain=act_drain,
    )
    ramp = SKEW * (zs - 1)
    steps = count + ramp
    todo = [(step, 0, z_step, (step,)) for step in range(steps)]
    todo += [(at, 1, acts[name], args) for at, name, *args in JOINS if n == 4 or name in ("share", "open", "join")]
    if n == 4:
        todo += [(ramp + at, 2, acts[name], args) for at, name, *args in TAIL]
    else:
        for at, name, *extra in PLAIN:
            for k in range(3):
                args = (k, *extra)
                todo.append((ramp + at + k * PIECES, 2, acts[name], args))
    for _, _, act, args in sorted(todo, key=lambda item: item[:2]):
        act(*args)

    if n != 4:
        act_drain()
    for k in range(3):
        if n != 4:
            bulk_all(k).wait_send()


def emit(*refs):
    copies = [pltpu.make_async_copy(refs[i], refs[15 + i], refs[30].at[i]) for i in range(15)]
    for cp in copies:
        cp.start()
    for cp in copies:
        cp.wait()


def shards(n, tp, *args):
    features = args[0]
    cots, bases, masters, firsts, seconds = (args[1 + i : 16 : 5] for i in range(5))
    tokens, width = features.shape
    rank = bases[0].shape[1]
    rows_dev = masters[0].shape[0]
    whole_rows = rows_dev * n
    half = tokens // 2
    count = 3 * PIECES
    piece = half // PIECES
    cols = [a.shape[1] for a in cots]

    outs = []
    for k in range(3):
        outs += [
            pltpu.VMEM(masters[k].shape, F32),
            pltpu.VMEM(masters[k].shape, F32),
            pltpu.VMEM(firsts[k].shape, F32),
            pltpu.VMEM(firsts[k].shape, F32),
            pltpu.VMEM((whole_rows, cols[k]), BF16),
        ]
    like = lambda arrays: [pltpu.VMEM(a.shape, a.dtype) for a in arrays]
    pairs = plan(n, rows_dev)
    wide = (n, rows_dev) if n == 4 else (1, 16)
    dma = lambda *shape: pltpu.SemaphoreType.DMA(shape)
    scratch = (
        [pltpu.VMEM((tokens, width), BF16), pltpu.VMEM((half, width), BF16)]
        + like(cots)
        + like(bases)
        + like(masters)
        + like(firsts)
        + like(seconds)
        + [pltpu.VMEM((count, piece, rank), F32)]
        + [pltpu.VMEM((count, piece, rank), BF16)] * 4
        + [pltpu.VMEM((3, half, rank), BF16)] * 2
        + [pltpu.VMEM((rank, w), F32) for w in cols]
        + [pltpu.VMEM((rank, w), BF16) for w in cols]
        + [pltpu.VMEM((n - 1, rank // n, w), BF16) for w in cols]
        + [pltpu.VMEM((rank, w), BF16) for w in cols]
        + [pltpu.VMEM((*wide, w), BF16) for w in cols]
        + [pltpu.VMEM((n, 1, w), F32) for w in cols]
        + [pltpu.VMEM((2 * rank, w), BF16) for w in cols]
        + [pltpu.VMEM((n, 1, 128 + w), F32) for w in cols]
        + [pltpu.VMEM((3, tp, 8, 128), F32)]
        + [dma(16), dma(2), dma(2, count), dma(2), dma(6 + SHARES)]
        + [dma(3)] * 3
        + [dma(3, 3)]
        + [dma(3)] * 4
        + [dma(1 if n == 4 else 3)] * 2
        + [dma(3), dma(max(len(pairs), 1), 2)]
        + [dma(3)] * 3
    )
    held = pl.pallas_call(
        functools.partial(kernel, n, tp),
        out_shape=outs,
        in_specs=[pl.BlockSpec(memory_space=pltpu.HBM)] * 16,
        out_specs=[pl.BlockSpec(memory_space=pltpu.VMEM)] * 15,
        scratch_shapes=scratch,
        compiler_params=pltpu.CompilerParams(
            collective_id=0, has_side_effects=True, vmem_limit_bytes=54 * 1024 * 1024
        ),
    )(*args)
    return pl.pallas_call(
        emit,
        out_shape=[jax.ShapeDtypeStruct(a.shape, a.dtype) for a in held],
        in_specs=[pl.BlockSpec(memory_space=pltpu.VMEM)] * 15,
        out_specs=[pl.BlockSpec(memory_space=pltpu.HBM)] * 15,
        scratch_shapes=[pltpu.SemaphoreType.DMA((15,))],
        compiler_params=pltpu.CompilerParams(vmem_limit_bytes=16 * 1024 * 1024),
    )(*held)


def solution(mesh):
    split = P("fs", "tp")
    return jax.shard_map(
        functools.partial(shards, mesh.shape["fs"], mesh.shape["tp"]),
        mesh=mesh,
        in_specs=(split,) + (split, P(), split, split, split) * 3,
        out_specs=(split, split, split, split, P(None, "tp")) * 3,
        check_vma=False,
    )
```
